32 devices in a mesh: grp: 2 (over x), st: 4 (over y, core), tp: 4 (over z).
Axes of the slice: x: 2, y: 2, z: 4, core: 2. Of those that a mesh axis runs over, the one named last changes fastest.
Arguments:
- tokens: bfloat16 [4096, 2048], P(('grp', 'st')), parts along dimension 0, may hold values from -6 to 6, as said below
- store: bfloat16 [64, 128, 2048], P(('grp', 'st')), parts along dimension 0, may hold values from -6 to 6, as said below
- passage_ids: int32 [64, 4], P(('grp', 'st')), parts along dimension 0, may hold values from 0 to 31, as said below
- mix_gain: float32 [2048], replicated, may hold values from 0.1 to 1.9
- glu_value: bfloat16 [2048, 1024], P(None, 'tp'), may hold values from -0.125 to 0.125
- glu_gate: bfloat16 [2048, 1024], P(None, 'tp'), may hold values from -0.125 to 0.125
- conv_taps: bfloat16 [31, 1024], P(None, 'tp'), may hold values from -5 to 5
- channel_gain: float32 [1024], P('tp'), may hold values from 0.1 to 1.9
- mix_out: bfloat16 [1024, 2048], P('tp'), may hold values from -0.1875 to 0.1875
- query_gain: float32 [2048], replicated, may hold values from 0.1 to 1.9
- passage_gain: float32 [2048], replicated, may hold values from 0.1 to 1.9
- query_proj: bfloat16 [2048, 2048], P(None, 'tp'), may hold values from -1 to 1
- key_proj: bfloat16 [2048, 2048], P(None, 'tp'), may hold values from -1 to 1
- value_proj: bfloat16 [2048, 2048], P(None, 'tp'), may hold values from -0.125 to 0.125
- attn_out: bfloat16 [2048, 2048], P('tp'), may hold values from -0.125 to 0.125
- blend_gain: float32 [2048], replicated, may hold values from 0.5 to 3
Outputs:
- blended: bfloat16 [4096, 2048], P(('grp', 'st', 'tp')), parts along dimension 0
The draws below stay inside these ranges and needn't reach their ends.
There are 2 independent parts, one for each index of `grp`. The reference program is written for one: setup_inputs(seed, part) draws one part's arguments, and reference() takes and returns one part's arrays. A program takes and returns all parts, laid end to end along the dimension named above; an argument that names none is the same for every part. Nothing has to cross between parts.
Inputs may be any that keep to these rules, and one draw needn't show every extreme that they name: `tokens`: standard normal entries clipped to the range. `store`: standard normal entries clipped to the range. `passage_ids`: passage p is held by index p // 8 of st. The 32 requests of the 8 blocks of one index of st (repeats counted) name at most 16 passages held by any one index of st, and in every draw one index of st receives exactly 16 requests from every index of st.
All inputs are finite; a program needn't handle non-finite values.
Results may differ from the reference program's by a relative error of at most 0.01575.
The reference program's roundings to bfloat16 on the way count: a program that leaves them out, or rounds other values in their place, can miss the bound.
Values may be sent and summed in bfloat16 or wider, within the bound.
A program may use at most 128 MiB of HBM per device.

```python
import jax
import jax.numpy as jnp
from jax import lax

D = 2048
CA = 1024
HEADS = 8
KW = 31
SEQ_LEN = 128
BLK = 64
NP = 4
PROWS = 128
PASS_DEV = 8
TOKENS = 2048
NB_DEV = 8
BLOCKS = 32
RQ = 32
MOST = 16
PASSAGES = 32
N_ST = 4
N_TP = 4


def request_table(key):
    hot_owner = jax.random.randint(jax.random.fold_in(key, 1), (), 0, N_ST)
    positions = jnp.arange(RQ)

    def one_device(device, dev_key):
        first_turn = (device - 1 - hot_owner) % N_ST - 1
        spread_turn = (first_turn + positions - MOST) % (N_ST - 1)
        owners_of = jnp.where(positions < MOST, hot_owner, (hot_owner + 1 + spread_turn) % N_ST)
        owners_of = owners_of[jax.random.permutation(dev_key, RQ)]
        local_index = jax.random.randint(jax.random.fold_in(dev_key, 3), (RQ,), 0, PASS_DEV)
        return (owners_of * PASS_DEV + local_index).reshape(NB_DEV, NP)
    dev_keys = jax.random.split(jax.random.fold_in(key, 2), N_ST)
    table = jax.vmap(one_device)(jnp.arange(N_ST), dev_keys)
    return table.reshape(BLOCKS, NP).astype(jnp.int32)


def store_rows(key):
    return jnp.clip(jax.random.normal(jax.random.fold_in(key, 12), (PASSAGES, PROWS, D), jnp.float32), -6.0, 6.0)


def draw_passage_ids(key, part):
    return request_table(jax.random.fold_in(key, 11))


def draw_store(key, part):
    return store_rows(key).astype(jnp.bfloat16)


def draw_tokens(key, part):
    plain_rows = jnp.clip(jax.random.normal(jax.random.fold_in(key, 13), (TOKENS, D), jnp.float32), -6.0, 6.0)
    return plain_rows.astype(jnp.bfloat16)


def draw_conv_taps(key, part):
    channel = jnp.arange(CA).astype(jnp.float32)
    channel_scale = jnp.exp(1.5 * (2.0 * channel / CA - 1.0)) * KW ** (-0.5)
    tap_draw = jnp.clip(jax.random.normal(jax.random.fold_in(key, 31), (KW, CA), jnp.float32), -6.0, 6.0)
    return jnp.clip(tap_draw * channel_scale, -5.0, 5.0).astype(jnp.bfloat16)


def draw_query_proj(key, part):
    fresh_draw = jax.random.normal(jax.random.fold_in(key, 22), (D, D), jnp.float32) * D ** (-0.5)
    return jnp.clip(fresh_draw, -1.0, 1.0).astype(jnp.bfloat16)


def draw_key_proj(key, part):
    fresh_draw = jax.random.normal(jax.random.fold_in(key, 23), (D, D), jnp.float32) * D ** (-0.5)
    return jnp.clip(fresh_draw, -1.0, 1.0).astype(jnp.bfloat16)


def shard_levels(stream_key, dims, pieces, smallest, high):
    gain, own = 1.0, jax.random.fold_in(stream_key, 6)
    for axis_at, blocks in pieces:
        steps = jnp.exp(jax.random.uniform(jax.random.fold_in(own, axis_at), (blocks,), jnp.float32, smallest / len(pieces), high / len(pieces)))
        gain = gain * jnp.repeat(steps, dims[axis_at] // blocks).reshape([-1 if axis == axis_at else 1 for axis in range(len(dims))])
    return gain


def normal_values(own_key, dims, scale, reach, cuts=(), dtype=jnp.bfloat16):
    drawn = jax.random.normal(own_key, dims, jnp.float32) * scale
    if len(cuts) > 0:
        drawn = shard_levels(own_key, dims, cuts, -0.22, 0.18) * drawn
    return jnp.clip(drawn, min=-reach, max=reach).astype(dtype)


def setup_inputs(seed: int = 0, part: int = 0) -> dict:
    streams_of = jax.random.split(jax.random.key(seed), 17)
    part_keys = jax.random.split(jax.random.fold_in(streams_of[16], part), 17)
    return {
        "tokens": draw_tokens(jax.random.fold_in(jax.random.fold_in(streams_of[16], part), 71), part),
        "store": draw_store(jax.random.fold_in(jax.random.fold_in(streams_of[16], part), 71), part),
        "passage_ids": draw_passage_ids(jax.random.fold_in(jax.random.fold_in(streams_of[16], part), 71), part),
        "mix_gain": jnp.clip(1.0 + 0.18 * jax.random.normal(streams_of[3], (D,), jnp.float32), 0.1, 1.9),
        "glu_value": normal_values(streams_of[4], (D, CA), D ** -0.5, 0.125, ((1, 4),)),
        "glu_gate": normal_values(streams_of[5], (D, CA), D ** -0.5, 0.125, ((1, 4),)),
        "conv_taps": draw_conv_taps(jax.random.fold_in(streams_of[16], 71), part),
        "channel_gain": jnp.clip(1.0 + 0.18 * jax.random.normal(streams_of[7], (CA,), jnp.float32), 0.1, 1.9),
        "mix_out": normal_values(streams_of[8], (CA, D), CA ** -0.5, 0.1875, ((0, 4),)),
        "query_gain": jnp.clip(1.0 + 0.18 * jax.random.normal(streams_of[9], (D,), jnp.float32), 0.1, 1.9),
        "passage_gain": jnp.clip(1.0 + 0.18 * jax.random.normal(streams_of[10], (D,), jnp.float32), 0.1, 1.9),
        "query_proj": draw_query_proj(jax.random.fold_in(streams_of[16], 71), part),
        "key_proj": draw_key_proj(jax.random.fold_in(streams_of[16], 71), part),
        "value_proj": normal_values(streams_of[13], (D, D), D ** -0.5, 0.125, ((1, 4),)),
        "attn_out": normal_values(streams_of[14], (D, D), D ** -0.5, 0.125, ((0, 4),)),
        "blend_gain": jnp.clip(jax.random.uniform(streams_of[15], (D,), jnp.float32, 0.5, 3.0), 0.5, 3.0),
    }


EPS = 1e-06

def rms_rows(row_data, gain_vec):
    floats = row_data.astype(jnp.float32)
    inv_scale = lax.rsqrt(lax.optimization_barrier(jnp.mean(floats * floats, axis=-1, keepdims=True)) + EPS)
    return (floats * inv_scale * gain_vec.astype(jnp.float32)).astype(jnp.bfloat16)

def depthwise(gated_rows, conv_taps):
    span_width = conv_taps.shape[0]
    half_span = (span_width - 1) // 2
    seq_length = gated_rows.shape[1]
    padded = jnp.pad(gated_rows.astype(jnp.float32), ((0, 0), (half_span, span_width - 1 - half_span), (0, 0)))
    running = jnp.zeros(gated_rows.shape, jnp.float32)
    for tap_index in range(span_width):
        running = running + padded[:, tap_index:tap_index + seq_length] * conv_taps[tap_index].astype(jnp.float32)
    return running

def passage_attention(queries, keys_values, head_count):
    groups, block_len, span_width = queries.shape
    head_dim = span_width // head_count
    row_count = keys_values.shape[1]
    query_heads = queries.astype(jnp.float32).reshape(groups, block_len, head_count, head_dim)
    key_heads = keys_values[:, :, :span_width].astype(jnp.float32).reshape(groups, row_count, head_count, head_dim)
    value_heads = keys_values[:, :, span_width:].astype(jnp.float32).reshape(groups, row_count, head_count, head_dim)
    scores = jnp.einsum('gqhd,grhd->ghqr', query_heads, key_heads) * head_dim ** (-0.5)
    row_top = lax.optimization_barrier(jnp.max(scores, axis=-1))
    exponent = jnp.exp(scores - row_top[..., None])
    row_sum = lax.optimization_barrier(jnp.sum(exponent, axis=-1))
    weights = exponent.astype(jnp.bfloat16).astype(jnp.float32)
    outputs = jnp.einsum('ghqr,grhd->gqhd', weights, value_heads).astype(jnp.bfloat16)
    return (outputs.reshape(groups, block_len, span_width), row_top, row_sum)

def combine(outs, tops, sums, head_count):
    batch_count, passage_count, block_len, span_width = outs.shape
    head_dim = span_width // head_count
    best_top = lax.optimization_barrier(jnp.max(tops, axis=1, keepdims=True))
    weight = jnp.exp(tops - best_top)
    numerator = jnp.einsum('bphq,bpqhd->bqhd', weight, outs.astype(jnp.float32).reshape(batch_count, passage_count, block_len, head_count, head_dim))
    denominator = lax.optimization_barrier(jnp.sum(weight * sums, axis=1))
    result = numerator / jnp.transpose(denominator, (0, 2, 1))[..., None]
    return result.reshape(batch_count, block_len, span_width).astype(jnp.bfloat16)

def reference(tokens, store, passage_ids, mix_gain, glu_value, glu_gate, conv_taps, channel_gain, mix_out, query_gain, passage_gain, query_proj, key_proj, value_proj, attn_out, blend_gain):
    mix_input = rms_rows(tokens, mix_gain)
    value_part = jnp.dot(mix_input, glu_value, preferred_element_type=jnp.float32)
    gate_part = jnp.dot(mix_input, glu_gate, preferred_element_type=jnp.float32)
    gated_rows = (value_part * jax.nn.sigmoid(gate_part)).astype(jnp.bfloat16)
    conv_rows = depthwise(gated_rows.reshape(-1, SEQ_LEN, CA), conv_taps).reshape(-1, CA)
    row_mean = lax.optimization_barrier(jnp.mean(conv_rows, axis=1, keepdims=True))
    row_var = lax.optimization_barrier(jnp.mean(conv_rows * conv_rows, axis=1, keepdims=True)) - row_mean * row_mean
    activation = jax.nn.silu((conv_rows - row_mean) * lax.rsqrt(row_var + EPS) * channel_gain.astype(jnp.float32)).astype(jnp.bfloat16)
    queries = jnp.dot(rms_rows(tokens, query_gain), query_proj, preferred_element_type=jnp.float32).astype(jnp.bfloat16)
    passage_rows = rms_rows(store.reshape(-1, D), passage_gain)
    key_rows = jnp.dot(passage_rows, key_proj, preferred_element_type=jnp.float32).astype(jnp.bfloat16)
    value_rows = jnp.dot(passage_rows, value_proj, preferred_element_type=jnp.float32).astype(jnp.bfloat16)
    memory = jnp.concatenate([key_rows, value_rows], axis=1).reshape(store.shape[0], store.shape[1], 2 * D)

    def one_block(inputs):
        block_queries, block_ids = inputs
        wanted = memory[block_ids]
        repeated = jnp.broadcast_to(block_queries[None], (NP, BLK, D))
        part_out, part_top, part_sum = passage_attention(repeated, wanted, HEADS)
        return combine(part_out[None], part_top[None], part_sum[None], HEADS)[0]
    attended = lax.map(one_block, (queries.reshape(-1, BLK, D), passage_ids)).reshape(-1, D)
    channel_group = CA // N_TP
    column_group = D // N_TP
    running = jnp.zeros((tokens.shape[0], D), jnp.float32)
    for shard_index in range(N_TP):
        conv_part = jnp.dot(activation[:, shard_index * channel_group:(shard_index + 1) * channel_group], mix_out[shard_index * channel_group:(shard_index + 1) * channel_group], preferred_element_type=jnp.float32)
        attn_part = jnp.dot(attended[:, shard_index * column_group:(shard_index + 1) * column_group], attn_out[shard_index * column_group:(shard_index + 1) * column_group], preferred_element_type=jnp.float32)
        partial_value = (conv_part + blend_gain.astype(jnp.float32) * attn_part).astype(jnp.bfloat16)
        partial_value = lax.optimization_barrier(partial_value)
        running = running + partial_value.astype(jnp.float32)
    return running.astype(jnp.bfloat16)
```

```python
import functools

import jax
import jax.numpy as jnp
from jax import lax
from jax.sharding import PartitionSpec as P
from jax.experimental import pallas as pl
from jax.experimental.pallas import tpu as pltpu

CA = 1024
HD = 256
SEQ_LEN = 128


EPS = 1e-06


def rms_rows(row_data, gain_vec):
    floats = row_data.astype(jnp.float32)
    inv_scale = lax.rsqrt(jnp.mean(floats * floats, axis=-1, keepdims=True) + EPS)
    return (floats * inv_scale * gain_vec).astype(jnp.bfloat16)


def depthwise(gated_rows, conv_taps):
    span_width = conv_taps.shape[0]
    half_span = (span_width - 1) // 2
    seq_length = gated_rows.shape[1]
    padded = jnp.pad(
        gated_rows.astype(jnp.float32), ((0, 0), (half_span, span_width - 1 - half_span), (0, 0))
    )
    running = jnp.zeros(gated_rows.shape, jnp.float32)
    for tap_index in range(span_width):
        running = running + padded[:, tap_index : tap_index + seq_length] * conv_taps[
            tap_index
        ].astype(jnp.float32)
    return running


def passage_attention(queries, keys_values, head_count):
    groups, block_len, span_width = queries.shape
    head_dim = span_width // head_count
    row_count = keys_values.shape[1]
    query_heads = queries.reshape(groups, block_len, head_count, head_dim)
    key_heads = keys_values[:, :, :span_width].reshape(groups, row_count, head_count, head_dim)
    value_heads = keys_values[:, :, span_width:].reshape(groups, row_count, head_count, head_dim)
    scores = jnp.einsum(
        "gqhd,grhd->ghqr", query_heads, key_heads, preferred_element_type=jnp.float32
    ) * head_dim ** (-0.5)
    row_top = jnp.max(scores, axis=-1)
    exponent = jnp.exp(scores - row_top[..., None])
    row_sum = jnp.sum(exponent, axis=-1)
    weights = exponent.astype(jnp.bfloat16)
    outputs = jnp.einsum(
        "ghqr,grhd->gqhd", weights, value_heads, preferred_element_type=jnp.float32
    ).astype(jnp.bfloat16)
    return (outputs.reshape(groups, block_len, span_width), row_top, row_sum)


def combine(outs, tops, sums, head_count):
    batch_count, passage_count, block_len, span_width = outs.shape
    head_dim = span_width // head_count
    best_top = jnp.max(tops, axis=1, keepdims=True)
    weight = jnp.exp(tops - best_top)
    numerator = jnp.einsum(
        "bphq,bpqhd->bqhd",
        weight,
        outs.astype(jnp.float32).reshape(
            batch_count, passage_count, block_len, head_count, head_dim
        ),
    )
    denominator = jnp.sum(weight * sums, axis=1)
    result = numerator / jnp.transpose(denominator, (0, 2, 1))[..., None]
    return result.reshape(batch_count, block_len, span_width).astype(jnp.bfloat16)


def local(
    tokens,
    store,
    passage_ids,
    mix_gain,
    glu_value,
    glu_gate,
    conv_taps,
    channel_gain,
    mix_out,
    query_gain,
    passage_gain,
    query_proj,
    key_proj,
    value_proj,
    attn_out,
    blend_gain,
):
    owners = lax.axis_size("st")
    tok_rows = tokens.shape[0]
    model_width = tokens.shape[1]
    local_channels = glu_value.shape[1]
    head_width = query_proj.shape[1]
    local_heads = head_width // HD
    block_count = passage_ids.shape[0]
    per_block = passage_ids.shape[1]
    block_len = tok_rows // block_count
    requests = block_count * per_block
    capacity = 2 * requests // owners
    pass_local = store.shape[0]
    pass_rows = store.shape[1]
    flat_ids = passage_ids.reshape(requests)
    owner_of = flat_ids // pass_local
    local_of = flat_ids - owner_of * pass_local
    request_index = jnp.arange(requests)
    earlier = (owner_of[:, None] == owner_of[None, :]) & (
        request_index[None, :] < request_index[:, None]
    )
    ranking = jnp.sum(earlier.astype(jnp.int32), axis=1)
    slot_of = owner_of * capacity + ranking
    slot_ids = (
        jnp.zeros((owners * capacity,), jnp.int32)
        .at[slot_of]
        .set(local_of)
        .reshape(owners, capacity)
    )
    asked = lax.all_to_all(slot_ids, "st", split_axis=0, concat_axis=0, tiled=True)
    normed_store = rms_rows(store.reshape(pass_local * pass_rows, model_width), passage_gain)
    key_rows = jnp.dot(normed_store, key_proj, preferred_element_type=jnp.float32).astype(
        jnp.bfloat16
    )
    value_rows = jnp.dot(normed_store, value_proj, preferred_element_type=jnp.float32).astype(
        jnp.bfloat16
    )
    memory = jnp.concatenate([key_rows, value_rows], axis=1).reshape(
        pass_local, pass_rows, 2 * head_width
    )
    queries = jnp.dot(
        rms_rows(tokens, query_gain), query_proj, preferred_element_type=jnp.float32
    ).astype(jnp.bfloat16)
    query_blocks = queries.reshape(block_count, block_len, head_width)
    repeated = jnp.repeat(query_blocks, per_block, axis=0)
    served = memory[asked.reshape(owners * capacity)]
    slot_queries = (
        jnp.zeros((owners * capacity, block_len, head_width), jnp.bfloat16)
        .at[slot_of]
        .set(repeated)
    )
    visiting = lax.all_to_all(
        slot_queries.reshape(owners, capacity, block_len, head_width),
        "st",
        split_axis=0,
        concat_axis=0,
        tiled=True,
    )
    answer_out, answer_top, answer_sum = passage_attention(
        visiting.reshape(owners * capacity, block_len, head_width), served, local_heads
    )
    back_out = lax.all_to_all(
        answer_out.reshape(owners, capacity, block_len, head_width),
        "st",
        split_axis=0,
        concat_axis=0,
        tiled=True,
    )
    back_top, back_sum = (
        lax.all_to_all(
            answer_top.reshape(owners, capacity, local_heads, block_len),
            "st",
            split_axis=0,
            concat_axis=0,
            tiled=True,
        ),
        lax.all_to_all(
            answer_sum.reshape(owners, capacity, local_heads, block_len),
            "st",
            split_axis=0,
            concat_axis=0,
            tiled=True,
        ),
    )
    partial_out = back_out.reshape(owners * capacity, block_len, head_width)[slot_of]
    partial_top = back_top.reshape(owners * capacity, local_heads, block_len)[slot_of]
    partial_sum = back_sum.reshape(owners * capacity, local_heads, block_len)[slot_of]
    attended = combine(
        partial_out.reshape(block_count, per_block, block_len, head_width),
        partial_top.reshape(block_count, per_block, local_heads, block_len),
        partial_sum.reshape(block_count, per_block, local_heads, block_len),
        local_heads,
    ).reshape(tok_rows, head_width)
    mix_input = rms_rows(tokens, mix_gain)
    value_part = jnp.dot(mix_input, glu_value, preferred_element_type=jnp.float32)
    gate_part = jnp.dot(mix_input, glu_gate, preferred_element_type=jnp.float32)
    gated_rows = (value_part * jax.nn.sigmoid(gate_part)).astype(jnp.bfloat16)
    conv_rows = depthwise(gated_rows.reshape(-1, SEQ_LEN, local_channels), conv_taps).reshape(
        tok_rows, local_channels
    )
    channel_sum, channel_square = lax.psum(
        (jnp.sum(conv_rows, axis=1), jnp.sum(conv_rows * conv_rows, axis=1)), "tp"
    )
    row_mean = channel_sum / CA
    row_var = channel_square / CA - row_mean * row_mean
    activation = jax.nn.silu(
        (conv_rows - row_mean[:, None]) * lax.rsqrt(row_var + EPS)[:, None] * channel_gain
    ).astype(jnp.bfloat16)
    conv_term = jnp.dot(activation, mix_out, preferred_element_type=jnp.float32)
    attn_term = jnp.dot(attended, attn_out, preferred_element_type=jnp.float32)
    return lax.psum_scatter(
        (conv_term + blend_gain * attn_term).astype(jnp.bfloat16),
        "tp",
        scatter_dimension=0,
        tiled=True,
    )


BF = jnp.bfloat16
F32 = jnp.float32
NEG = -3e38
VMEM_MIB = 60


def mm(a, b):
    return jnp.dot(a, b, preferred_element_type=F32)


def wait_in(ref, sem):
    pltpu.make_async_copy(ref, ref, sem).wait()


def layer_kernel(
    n_st, n_tp, block_count, per_block, block_len, local_heads, seq_len, pass_rows,
    tokens_h, store_h, ids_h, mix_h, gv_h, gg_h, taps_h, channel_h, mo_h, query_h,
    passage_h, qw_h, kw_h, vw_h, ao_h, blend_h,
    out_ref,
    tok, sto, gv, gg, mo, qw, kw, vw, ao, load_sem,
    ids_v, mix_gain, taps, channel_gain, query_gain, passage_gain, blend_gain, small_sem,
    ids_all, ids_s, ids_send, ids_recv, ids_sem,
    q_all, q_stage, q_send, q_recv,
    k_all, v_all, k_stage, v_stage, kv_send, kv_recv,
    gp, conv, scol, stat_all, stat_send, stat_recv, act,
    out_o, out_s, ret_o, ret_s, o_send, o_recv, s_send, s_recv,
    part, from_left, from_right, r_send, r_recv,
):
    st = lax.axis_index("st")
    tp = lax.axis_index("tp")
    core = lax.rem(st, 2)
    chip = st // 2
    n_chip = n_st // 2
    other = 1 - core
    T = tok.shape[0]
    R = sto.shape[0]
    HW = q_stage.shape[1]
    CL = act.shape[1]

    smalls = []
    for n, (a, b) in enumerate(
        [(query_h, query_gain), (mix_h, mix_gain), (ids_h, ids_v), (passage_h, passage_gain), (taps_h, taps),
         (channel_h, channel_gain), (blend_h, blend_gain)]
    ):
        c = pltpu.make_async_copy(a, b, small_sem.at[n])
        c.start()
        smalls.append(c)
    loads = []
    for n, (a, b) in enumerate(
        [(tokens_h, tok), (qw_h, qw), (store_h, sto), (kw_h, kw), (vw_h, vw), (gv_h, gv),
         (gg_h, gg), (mo_h, mo), (ao_h, ao)]
    ):
        c = pltpu.make_async_copy(a, b, load_sem.at[n])
        c.start()
        loads.append(c)

    barrier = pltpu.get_barrier_semaphore()
    for i in range(1, n_st):
        pl.semaphore_signal(barrier, inc=1, device_id={"st": lax.rem(st + i, n_st)},
                            device_id_type=pl.DeviceIdType.MESH)
    for i in range(1, n_tp):
        pl.semaphore_signal(barrier, inc=1, device_id={"tp": lax.rem(tp + i, n_tp)},
                            device_id_type=pl.DeviceIdType.MESH)

    def remote(src, dst, ssem, rsem, axis, to):
        return pltpu.make_async_remote_copy(
            src_ref=src, dst_ref=dst, send_sem=ssem, recv_sem=rsem, device_id={axis: to},
            device_id_type=pl.DeviceIdType.MESH)

    chunk_rows = T // n_tp
    table = [sorted(range(n_tp), key=lambda d: -abs(d - t)) for t in range(n_tp)]

    def chunk_at(k):
        d = jnp.int32(table[0][k])
        for t in range(1, n_tp):
            d = jnp.where(tp == t, table[t][k], d)
        return d

    chunks = [chunk_at(k) for k in range(n_tp)]

    def chunk_ds(d):
        return pl.ds(pl.multiple_of(d * chunk_rows, chunk_rows), chunk_rows)

    def peers():
        res = [(chip * 2 + other, True, 0)]
        for j in range(1, n_chip):
            c = lax.rem(chip + j, n_chip)
            res.append((c * 2 + core, False, 2 * j - 1))
            res.append((c * 2 + other, True, 2 * j))
        return res

    for c in smalls:
        c.wait()
    loads[0].wait()
    loads[1].wait()
    TC = 256
    mine = pl.ds(pl.multiple_of(core * HW, HW), HW)
    theirs = pl.ds(pl.multiple_of(other * HW, HW), HW)

    def tok_chunk(i, carry):
        rows = pl.ds(pl.multiple_of(i * TC, TC), TC)
        x = tok[rows, :].astype(F32)
        y = x * lax.rsqrt(jnp.mean(x * x, axis=-1, keepdims=True) + EPS)
        qr = (y * query_gain[...]).astype(BF)
        q_all[st, rows, :] = mm(qr, qw[:, mine]).astype(BF)
        q_stage[rows, :] = mm(qr, qw[:, theirs]).astype(BF)
        tok[rows, :] = (y * mix_gain[...]).astype(BF)
        return carry

    lax.fori_loop(0, T // TC, tok_chunk, 0)

    pl.semaphore_wait(barrier, n_st - 1 + n_tp - 1)
    for i in range(1, n_st):
        remote(ids_v, ids_all.at[st], ids_send.at[i], ids_recv.at[st], "st",
               lax.rem(st + i, n_st)).start()
    ids_own = pltpu.make_async_copy(ids_v, ids_all.at[st], ids_recv.at[st])
    ids_own.start()

    def q_copies(k):
        rows = chunk_ds(chunks[k])
        for to, stage, n in peers():
            src = q_stage.at[rows] if stage else q_all.at[st, rows]
            yield remote(src, q_all.at[st, rows], q_send.at[n, k], q_recv.at[st, k], "st", to)

    for k in range(n_tp):
        for c in q_copies(k):
            c.start()

    for n in range(2, 5):
        loads[n].wait()
    RC = 512
    n_rc = R // RC
    RP = RC // pass_rows
    pass_local = R // pass_rows
    partner = chip * 2 + other

    def store_chunk(i, carry):
        rows = pl.ds(pl.multiple_of(i * RC, RC), RC)
        x = sto[rows, :].astype(F32)
        n = (x * lax.rsqrt(jnp.mean(x * x, axis=-1, keepdims=True) + EPS) * passage_gain[...]).astype(BF)
        here, slots = pl.ds(i * RP, RP), pl.ds(core * pass_local + i * RP, RP)
        k_stage[here] = mm(n, kw[:, theirs]).astype(BF).reshape(RP, pass_rows, HW)
        v_stage[here] = mm(n, vw[:, theirs]).astype(BF).reshape(RP, pass_rows, HW)
        remote(k_stage.at[here], k_all.at[slots], kv_send.at[0, i], kv_recv.at[0, i], "st", partner).start()
        remote(v_stage.at[here], v_all.at[slots], kv_send.at[1, i], kv_recv.at[1, i], "st", partner).start()
        k_all[slots] = mm(n, kw[:, mine]).astype(BF).reshape(RP, pass_rows, HW)
        v_all[slots] = mm(n, vw[:, mine]).astype(BF).reshape(RP, pass_rows, HW)
        return carry

    lax.fori_loop(0, n_rc, store_chunk, 0)

    ids_own.wait()
    for i in range(1, n_st):
        r = lax.rem(st + i, n_st)
        remote(ids_v, ids_all.at[r], ids_send.at[i], ids_recv.at[r], "st", r).wait_recv()
    c = pltpu.make_async_copy(ids_all, ids_s, ids_sem)
    c.start()
    c.wait()

    def kv_wait(i, carry):
        here, slots = pl.ds(i * RP, RP), pl.ds(other * pass_local + i * RP, RP)
        remote(k_stage.at[here], k_all.at[slots], kv_send.at[0, i], kv_recv.at[0, i], "st", partner).wait()
        remote(v_stage.at[here], v_all.at[slots], kv_send.at[1, i], kv_recv.at[1, i], "st", partner).wait()
        return carry

    lax.fori_loop(0, n_rc, kv_wait, 0)

    heads = local_heads // 2
    HD_ = HW // heads
    per_chip = 2 * pass_local
    chunk_blocks = block_count // n_tp
    clane = lax.broadcasted_iota(jnp.int32, (chunk_rows, 128), 1)
    scale = HD_ ** (-0.5)

    def order(i):
        return lax.rem(chip + 1 + i // 2, n_chip) * 2 + lax.rem(core + 1 - i % 2, 2)

    def answer_copies(k, r):
        rows = chunk_ds(chunks[k])
        return (
            remote(out_o.at[r, rows], ret_o.at[st, rows], o_send.at[r, k], o_recv.at[st, k], "st", r),
            remote(out_s.at[r, k], ret_s.at[st, k], s_send.at[r, k], s_recv.at[st, k], "st", r),
        )

    def attend(k):
        d = chunks[k]
        rows = chunk_ds(d)

        def pair(g, carry):
            rs = [order(2 * g), order(2 * g + 1)]
            for e, r in enumerate(rs):
                @pl.when(jnp.logical_or(e == 0, g < n_chip - 1))
                def _(r=r):
                    remote(q_all.at[st, rows], q_all.at[r, rows], q_send.at[0, k], q_recv.at[r, k], "st", r).wait_recv()

            units = [(e, h, u) for e in range(2) for h in range(heads) for u in range(chunk_blocks)]
            place, values, scores = {}, {}, {}
            for e, h, u in units:
                r = rs[e]
                cols = slice(h * HD_, (h + 1) * HD_)
                b = d * chunk_blocks + u
                brow = pl.ds(pl.multiple_of(b * block_len, block_len), block_len)
                ks, vs, bias = [], [], []
                for j in range(per_block):
                    p = ids_s[r, j, b] - chip * per_chip
                    spread_p = jnp.full((1, pass_rows), p, jnp.int32)
                    valid = jnp.logical_and(spread_p >= 0, spread_p < per_chip)
                    bias.append(jnp.where(valid, 0.0, NEG))
                    slot = jnp.clip(p, 0, per_chip - 1)
                    ks.append(k_all[slot][:, cols])
                    vs.append(v_all[slot][:, cols])
                s = lax.dot_general(q_all[r, brow, cols], jnp.concatenate(ks, axis=0), (((1,), (1,)), ((), ())),
                                    preferred_element_type=F32)
                scores[e, h, u] = s * scale + jnp.concatenate(bias, axis=1)
                values[e, h, u] = jnp.concatenate(vs, axis=0)
                place[e, h, u] = (r, brow, cols)
            tops = {n: jnp.maximum(jnp.max(scores[n], axis=1, keepdims=True), NEG / 2) for n in units}
            weights, dens = {}, {}
            for n in units:
                exponent = jnp.exp(scores[n] - tops[n])
                dens[n] = jnp.sum(exponent, axis=1, keepdims=True)
                weights[n] = exponent.astype(BF)
            for n in units:
                r, brow, cols = place[n]
                out_o[r, brow, cols] = mm(weights[n], values[n]).astype(BF)
            stats = jnp.zeros((chunk_rows, 128), F32)
            for e in range(2):
                for h in range(heads):
                    for at, parts in ((2 * h, tops), (2 * h + 1, dens)):
                        column = jnp.concatenate([parts[e, h, u] for u in range(chunk_blocks)], axis=0)
                        stats = jnp.where(clane == 8 * e + at, column, stats)
            turned = jnp.transpose(stats)
            for e, r in enumerate(rs):
                out_s[r, k] = turned[8 * e:8 * e + 8]

                @pl.when(jnp.logical_or(e == 0, g < n_chip - 1))
                def _(r=r):
                    for c in answer_copies(k, r):
                        c.start()

            return carry

        lax.fori_loop(0, n_chip, pair, 0)

    attend(0)

    loads[5].wait()
    loads[6].wait()
    per_seq = seq_len
    pad = (gp.shape[1] - per_seq) // 2
    gp[:, :pad] = jnp.zeros((gp.shape[0], pad, CL), F32)
    gp[:, pad + per_seq:] = jnp.zeros((gp.shape[0], pad, CL), F32)

    def glu_chunk(i, carry):
        mr = tok[pl.ds(pl.multiple_of(i * TC, TC), TC), :]
        gated = (mm(mr, gv[...]) * jax.nn.sigmoid(mm(mr, gg[...]))).astype(BF).astype(F32)
        for u in range(TC // per_seq):
            gp[i * (TC // per_seq) + u, pad:pad + per_seq, :] = gated[u * per_seq:(u + 1) * per_seq]
        return carry

    lax.fori_loop(0, T // TC, glu_chunk, 0)
    tap_values = taps[...].astype(F32)
    n_tap = taps.shape[0]
    lead = pad - (n_tap - 1) // 2
    CC = 64
    per = per_seq // CC
    lane = lax.broadcasted_iota(jnp.int32, (CC, 128), 1)

    def conv_chunk(i, carry):
        seq = i // per
        base = pl.multiple_of(lax.rem(i, per) * CC, CC)
        win = gp[seq, pl.ds(base, CC + 2 * pad), :]
        acc = None
        for res in range(8):
            group = None
            for k in range(n_tap):
                if (lead + k) % 8 == res:
                    at = lead + k - res
                    term = win[at:at + CC + (8 if res else 0)] * tap_values[k:k + 1]
                    group = term if group is None else group + term
            if group is not None:
                group = group[res:res + CC]
                acc = group if acc is None else acc + group
        rows = pl.ds(pl.multiple_of(i * CC, CC), CC)
        conv[rows, :] = acc
        s = jnp.sum(acc, axis=1, keepdims=True)
        ss = jnp.sum(acc * acc, axis=1, keepdims=True)
        scol[rows, :] = jnp.where(lane == 0, s, jnp.where(lane == 1, ss, 0.0))
        return carry

    lax.fori_loop(0, T // CC, conv_chunk, 0)
    stat_all[tp] = jnp.transpose(scol[...])[:8]
    for i in range(1, n_tp):
        remote(stat_all.at[tp], stat_all.at[tp], stat_send.at[i], stat_recv.at[tp], "tp",
               lax.rem(tp + i, n_tp)).start()

    attend(1)

    total = stat_all[tp]
    for i in range(1, n_tp):
        r = lax.rem(tp + i, n_tp)
        remote(stat_all.at[tp], stat_all.at[r], stat_send.at[i], stat_recv.at[r], "tp", r).wait_recv()
        total = total + stat_all[r]
    ca = CL * n_tp
    mean = total / ca
    spread = jnp.transpose(jnp.concatenate([mean, jnp.zeros((120, T), F32)], axis=0))
    row_mean = spread[:, 0:1]
    inv = lax.rsqrt(spread[:, 1:2] - row_mean * row_mean + EPS)
    a = (conv[...] - row_mean) * inv * channel_gain[...]
    act[...] = (a / (1.0 + jnp.exp(-a))).astype(BF)
    loads[7].wait()
    loads[8].wait()

    SUB = 4
    SR = chunk_rows // SUB

    def hop(k, u, ahead, buf, way):
        d = chunks[k]
        prow = pl.ds(pl.multiple_of(d * chunk_rows + u * SR, SR), SR)
        brow = pl.ds(u * SR, SR)
        to = jnp.clip(tp + ahead, 0, n_tp - 1)
        return prow, brow, remote(part.at[prow], buf.at[d, brow], r_send.at[way, d, u],
                                  r_recv.at[way, d, u], "tp", to)

    ways = ((1, from_left, 0), (-1, from_right, 1))

    def goes(k, way):
        return tp < chunks[k] if way == 0 else tp > chunks[k]

    def at_end(way):
        return tp == 0 if way == 0 else tp == n_tp - 1

    def finish(k):
        rows = chunk_ds(chunks[k])
        for i in range(n_st - 1):
            r = order(i)
            remote(out_o.at[r, rows], ret_o.at[r, rows], o_send.at[r, k], o_recv.at[r, k], "st", r).wait_recv()
            remote(out_s.at[r, k], ret_s.at[r, k], s_send.at[r, k], s_recv.at[r, k], "st", r).wait_recv()
        ret_o[st, rows, :] = out_o[st, rows, :]
        ret_s[st, k] = out_s[st, k]
        stats = jnp.transpose(jnp.concatenate(
            [ret_s[c, k] for c in range(n_st)] + [jnp.zeros((128 - 8 * n_st, chunk_rows), F32)], axis=0))
        pieces = []
        for g in range(2):
            for h in range(heads):
                cols = slice(h * HD_, (h + 1) * HD_)
                at = [8 * (c * 2 + g) + 2 * h for c in range(n_chip)]
                best = functools.reduce(jnp.maximum, [stats[:, x:x + 1] for x in at])
                num, den = 0.0, 0.0
                for c in range(n_chip):
                    w = jnp.exp(stats[:, at[c]:at[c] + 1] - best)
                    num = num + w * ret_o[c * 2 + g, rows, cols].astype(F32)
                    den = den + w * stats[:, at[c] + 1:at[c] + 2]
                pieces.append((num / den).astype(BF))
        attended = jnp.concatenate(pieces, axis=1)
        act_rows = act[rows, :]
        NC = 512
        for i in range(part.shape[1] // NC):
            cols = slice(i * NC, (i + 1) * NC)
            value = mm(act_rows, mo[:, cols]) + blend_gain[:, cols] * mm(attended, ao[:, cols])
            part[rows, cols] = value.astype(BF)
        if k < n_tp - 1:
            for ahead, buf, way in ways:
                @pl.when(jnp.logical_and(goes(k, way), at_end(way)))
                def _(ahead=ahead, buf=buf, way=way):
                    for u in range(SUB):
                        hop(k, u, ahead, buf, way)[2].start()

    def forward(k, u):
        for ahead, buf, way in ways:
            @pl.when(jnp.logical_and(goes(k, way), jnp.logical_not(at_end(way))))
            def _(ahead=ahead, buf=buf, way=way):
                prow, brow, copy = hop(k, u, ahead, buf, way)
                copy.wait_recv()
                part[prow, :] = (part[prow, :].astype(F32) + buf[chunks[k], brow, :].astype(F32)).astype(BF)
                copy.start()

    forwarded = 0
    for k in range(n_tp):
        finish(k)
        if k + 2 < n_tp:
            attend(k + 2)
        elif k < n_tp - 1:
            for u in range(SUB):
                forward(k - 2, u)
            forwarded = k - 1
    for u in range(SUB):
        for k in range(forwarded, n_tp - 1):
            forward(k, u)

    for u in range(SUB):
        prow = pl.ds(pl.multiple_of(tp * chunk_rows + u * SR, SR), SR)
        brow = pl.ds(u * SR, SR)

        for ahead, buf, way in ways:
            @pl.when(jnp.logical_not(at_end(way)))
            def _(buf=buf, way=way, ahead=ahead):
                to = jnp.clip(tp - ahead, 0, n_tp - 1)
                remote(part.at[prow], buf.at[tp, brow], r_send.at[way, tp, u], r_recv.at[way, tp, u], "tp",
                       to).wait_recv()

            @pl.when(at_end(way))
            def _(buf=buf):
                buf[tp, brow, :] = jnp.zeros((SR, part.shape[1]), BF)

        out_ref[brow, :] = (
            part[prow, :].astype(F32) + from_left[tp, brow, :].astype(F32) + from_right[tp, brow, :].astype(F32)
        ).astype(BF)

    for i in range(1, n_st):
        r = lax.rem(st + i, n_st)
        remote(ids_v, ids_all.at[st], ids_send.at[i], ids_recv.at[st], "st", r).wait_send()
    for k in range(n_tp):
        for c in q_copies(k):
            c.wait_send()
        for i in range(n_st - 1):
            for c in answer_copies(k, order(i)):
                c.wait_send()
    for i in range(1, n_tp):
        remote(stat_all.at[tp], stat_all.at[tp], stat_send.at[i], stat_recv.at[tp], "tp",
               lax.rem(tp + i, n_tp)).wait_send()
    for k in range(n_tp - 1):
        for ahead, buf, way in ways:
            @pl.when(goes(k, way))
            def _(ahead=ahead, buf=buf, way=way):
                for u in range(SUB):
                    hop(k, u, ahead, buf, way)[2].wait_send()


def fused_local(
    tokens, store, passage_ids, mix_gain, glu_value, glu_gate, conv_taps, channel_gain, mix_out,
    query_gain, passage_gain, query_proj, key_proj, value_proj, attn_out, blend_gain,
):
    n_st = lax.axis_size("st")
    n_tp = lax.axis_size("tp")
    T, D = tokens.shape
    P_, PR, _ = store.shape
    R = P_ * PR
    W = query_proj.shape[1]
    HW = W // 2
    CL = glu_value.shape[1]
    nb, per_block = passage_ids.shape
    pad = 8 * pl.cdiv((conv_taps.shape[0] - 1) // 2, 8)
    DMA = pltpu.SemaphoreType.DMA
    V = pltpu.VMEM
    SUB = 4
    kern = functools.partial(layer_kernel, n_st, n_tp, nb, per_block, T // nb, W // HD, SEQ_LEN, PR)
    hbm = pl.BlockSpec(memory_space=pl.ANY)
    vm = pl.BlockSpec(memory_space=pltpu.VMEM)
    return pl.pallas_call(
        kern,
        out_shape=pltpu.VMEM((T // n_tp, D), BF),
        in_specs=[hbm] * 16,
        out_specs=vm,
        scratch_shapes=[
            V((T, D), BF), V((R, D), BF), V((D, CL), BF), V((D, CL), BF), V((CL, D), BF),
            V((D, W), BF), V((D, W), BF), V((D, W), BF), V((W, D), BF), DMA((9,)),
            V((per_block, nb), jnp.int32), V((1, D), F32), V(conv_taps.shape, BF), V((1, CL), F32), V((1, D), F32),
            V((1, D), F32), V((1, D), F32), DMA((7,)),
            V((n_st, per_block, nb), jnp.int32), pltpu.SMEM((n_st, per_block, nb), jnp.int32),
            DMA((n_st,)), DMA((n_st,)), DMA,
            V((n_st, T, HW), BF), V((T, HW), BF), DMA((n_st - 1, n_tp)), DMA((n_st, n_tp)),
            V((2 * P_, PR, HW), BF), V((2 * P_, PR, HW), BF), V((P_, PR, HW), BF), V((P_, PR, HW), BF),
            DMA((2, R // 512)), DMA((2, R // 512)),
            V((T // SEQ_LEN, SEQ_LEN + 2 * pad, CL), F32), V((T, CL), F32), V((T, 128), F32),
            V((n_tp, 8, T), F32), DMA((n_tp,)), DMA((n_tp,)), V((T, CL), BF),
            V((n_st, T, HW), BF), V((n_st, n_tp, 8, T // n_tp), F32), V((n_st, T, HW), BF),
            V((n_st, n_tp, 8, T // n_tp), F32),
            DMA((n_st, n_tp)), DMA((n_st, n_tp)), DMA((n_st, n_tp)), DMA((n_st, n_tp)),
            V((T, D), BF), V((n_tp, T // n_tp, D), BF), V((n_tp, T // n_tp, D), BF),
            DMA((2, n_tp, SUB)), DMA((2, n_tp, SUB)),
        ],
        compiler_params=pltpu.CompilerParams(
            collective_id=0, has_side_effects=True, vmem_limit_bytes=VMEM_MIB * 1024 * 1024),
        name="layer",
    )(
        tokens, store.reshape(R, D), passage_ids.T, mix_gain.reshape(1, D), glu_value, glu_gate, conv_taps,
        channel_gain.reshape(1, CL), mix_out, query_gain.reshape(1, D), passage_gain.reshape(1, D),
        query_proj, key_proj, value_proj, attn_out, blend_gain.reshape(1, D),
    )


def solution(mesh):
    in_specs = (
        P(("grp", "st"), None),
        P(("grp", "st"), None, None),
        P(("grp", "st"), None),
        P(),
        P(None, "tp"),
        P(None, "tp"),
        P(None, "tp"),
        P("tp"),
        P("tp", None),
        P(),
        P(),
        P(None, "tp"),
        P(None, "tp"),
        P(None, "tp"),
        P("tp", None),
        P(),
    )
    out_specs = P(("grp", "st", "tp"), None)
    def body(*args):
        even = args[11].shape[1] // HD % 2 == 0 and mesh.shape["st"] % 2 == 0
        even = even and args[2].shape[0] % mesh.shape["tp"] == 0 and mesh.shape["st"] <= 16
        return (fused_local if even else local)(*args)

    return jax.shard_map(body, mesh=mesh, in_specs=in_specs, out_specs=out_specs, check_vma=False)
```

```python
import functools

import jax
import jax.numpy as jnp
from jax import lax
from jax.sharding import PartitionSpec as P
from jax.experimental import pallas as pl
from jax.experimental.pallas import tpu as pltpu

CA = 1024
HD = 256
SEQ_LEN = 128


EPS = 1e-06


def rms_rows(row_data, gain_vec):
    floats = row_data.astype(jnp.float32)
    inv_scale = lax.rsqrt(jnp.mean(floats * floats, axis=-1, keepdims=True) + EPS)
    return (floats * inv_scale * gain_vec).astype(jnp.bfloat16)


def depthwise(gated_rows, conv_taps):
    span_width = conv_taps.shape[0]
    half_span = (span_width - 1) // 2
    seq_length = gated_rows.shape[1]
    padded = jnp.pad(
        gated_rows.astype(jnp.float32), ((0, 0), (half_span, span_width - 1 - half_span), (0, 0))
    )
    running = jnp.zeros(gated_rows.shape, jnp.float32)
    for tap_index in range(span_width):
        running = running + padded[:, tap_index : tap_index + seq_length] * conv_taps[
            tap_index
        ].astype(jnp.float32)
    return running


def passage_attention(queries, keys_values, head_count):
    groups, block_len, span_width = queries.shape
    head_dim = span_width // head_count
    row_count = keys_values.shape[1]
    query_heads = queries.reshape(groups, block_len, head_count, head_dim)
    key_heads = keys_values[:, :, :span_width].reshape(groups, row_count, head_count, head_dim)
    value_heads = keys_values[:, :, span_width:].reshape(groups, row_count, head_count, head_dim)
    scores = jnp.einsum(
        "gqhd,grhd->ghqr", query_heads, key_heads, preferred_element_type=jnp.float32
    ) * head_dim ** (-0.5)
    row_top = jnp.max(scores, axis=-1)
    exponent = jnp.exp(scores - row_top[..., None])
    row_sum = jnp.sum(exponent, axis=-1)
    weights = exponent.astype(jnp.bfloat16)
    outputs = jnp.einsum(
        "ghqr,grhd->gqhd", weights, value_heads, preferred_element_type=jnp.float32
    ).astype(jnp.bfloat16)
    return (outputs.reshape(groups, block_len, span_width), row_top, row_sum)


def combine(outs, tops, sums, head_count):
    batch_count, passage_count, block_len, span_width = outs.shape
    head_dim = span_width // head_count
    best_top = jnp.max(tops, axis=1, keepdims=True)
    weight = jnp.exp(tops - best_top)
    numerator = jnp.einsum(
        "bphq,bpqhd->bqhd",
        weight,
        outs.astype(jnp.float32).reshape(
            batch_count, passage_count, block_len, head_count, head_dim
        ),
    )
    denominator = jnp.sum(weight * sums, axis=1)
    result = numerator / jnp.transpose(denominator, (0, 2, 1))[..., None]
    return result.reshape(batch_count, block_len, span_width).astype(jnp.bfloat16)


def local(
    tokens,
    store,
    passage_ids,
    mix_gain,
    glu_value,
    glu_gate,
    conv_taps,
    channel_gain,
    mix_out,
    query_gain,
    passage_gain,
    query_proj,
    key_proj,
    value_proj,
    attn_out,
    blend_gain,
):
    owners = lax.axis_size("st")
    tok_rows = tokens.shape[0]
    model_width = tokens.shape[1]
    local_channels = glu_value.shape[1]
    head_width = query_proj.shape[1]
    local_heads = head_width // HD
    block_count = passage_ids.shape[0]
    per_block = passage_ids.shape[1]
    block_len = tok_rows // block_count
    requests = block_count * per_block
    capacity = 2 * requests // owners
    pass_local = store.shape[0]
    pass_rows = store.shape[1]
    flat_ids = passage_ids.reshape(requests)
    owner_of = flat_ids // pass_local
    local_of = flat_ids - owner_of * pass_local
    request_index = jnp.arange(requests)
    earlier = (owner_of[:, None] == owner_of[None, :]) & (
        request_index[None, :] < request_index[:, None]
    )
    ranking = jnp.sum(earlier.astype(jnp.int32), axis=1)
    slot_of = owner_of * capacity + ranking
    slot_ids = (
        jnp.zeros((owners * capacity,), jnp.int32)
        .at[slot_of]
        .set(local_of)
        .reshape(owners, capacity)
    )
    asked = lax.all_to_all(slot_ids, "st", split_axis=0, concat_axis=0, tiled=True)
    normed_store = rms_rows(store.reshape(pass_local * pass_rows, model_width), passage_gain)
    key_rows = jnp.dot(normed_store, key_proj, preferred_element_type=jnp.float32).astype(
        jnp.bfloat16
    )
    value_rows = jnp.dot(normed_store, value_proj, preferred_element_type=jnp.float32).astype(
        jnp.bfloat16
    )
    memory = jnp.concatenate([key_rows, value_rows], axis=1).reshape(
        pass_local, pass_rows, 2 * head_width
    )
    queries = jnp.dot(
        rms_rows(tokens, query_gain), query_proj, preferred_element_type=jnp.float32
    ).astype(jnp.bfloat16)
    query_blocks = queries.reshape(block_count, block_len, head_width)
    repeated = jnp.repeat(query_blocks, per_block, axis=0)
    served = memory[asked.reshape(owners * capacity)]
    slot_queries = (
        jnp.zeros((owners * capacity, block_len, head_width), jnp.bfloat16)
        .at[slot_of]
        .set(repeated)
    )
    visiting = lax.all_to_all(
        slot_queries.reshape(owners, capacity, block_len, head_width),
        "st",
        split_axis=0,
        concat_axis=0,
        tiled=True,
    )
    answer_out, answer_top, answer_sum = passage_attention(
        visiting.reshape(owners * capacity, block_len, head_width), served, local_heads
    )
    back_out = lax.all_to_all(
        answer_out.reshape(owners, capacity, block_len, head_width),
        "st",
        split_axis=0,
        concat_axis=0,
        tiled=True,
    )
    back_top, back_sum = (
        lax.all_to_all(
            answer_top.reshape(owners, capacity, local_heads, block_len),
            "st",
            split_axis=0,
            concat_axis=0,
            tiled=True,
        ),
        lax.all_to_all(
            answer_sum.reshape(owners, capacity, local_heads, block_len),
            "st",
            split_axis=0,
            concat_axis=0,
            tiled=True,
        ),
    )
    partial_out = back_out.reshape(owners * capacity, block_len, head_width)[slot_of]
    partial_top = back_top.reshape(owners * capacity, local_heads, block_len)[slot_of]
    partial_sum = back_sum.reshape(owners * capacity, local_heads, block_len)[slot_of]
    attended = combine(
        partial_out.reshape(block_count, per_block, block_len, head_width),
        partial_top.reshape(block_count, per_block, local_heads, block_len),
        partial_sum.reshape(block_count, per_block, local_heads, block_len),
        local_heads,
    ).reshape(tok_rows, head_width)
    mix_input = rms_rows(tokens, mix_gain)
    value_part = jnp.dot(mix_input, glu_value, preferred_element_type=jnp.float32)
    gate_part = jnp.dot(mix_input, glu_gate, preferred_element_type=jnp.float32)
    gated_rows = (value_part * jax.nn.sigmoid(gate_part)).astype(jnp.bfloat16)
    conv_rows = depthwise(gated_rows.reshape(-1, SEQ_LEN, local_channels), conv_taps).reshape(
        tok_rows, local_channels
    )
    channel_sum, channel_square = lax.psum(
        (jnp.sum(conv_rows, axis=1), jnp.sum(conv_rows * conv_rows, axis=1)), "tp"
    )
    row_mean = channel_sum / CA
    row_var = channel_square / CA - row_mean * row_mean
    activation = jax.nn.silu(
        (conv_rows - row_mean[:, None]) * lax.rsqrt(row_var + EPS)[:, None] * channel_gain
    ).astype(jnp.bfloat16)
    conv_term = jnp.dot(activation, mix_out, preferred_element_type=jnp.float32)
    attn_term = jnp.dot(attended, attn_out, preferred_element_type=jnp.float32)
    return lax.psum_scatter(
        (conv_term + blend_gain * attn_term).astype(jnp.bfloat16),
        "tp",
        scatter_dimension=0,
        tiled=True,
    )


BF = jnp.bfloat16
F32 = jnp.float32
NEG = -3e38
VMEM_MIB = 60
PRIO = 1


def mm(a, b):
    return jnp.dot(a, b, preferred_element_type=F32)


def wait_in(ref, sem):
    pltpu.make_async_copy(ref, ref, sem).wait()


def layer_kernel(
    n_st, n_tp, block_count, per_block, block_len, local_heads, seq_len, pass_rows,
    tokens_h, store_h, ids_h, mix_h, gv_h, gg_h, taps_h, channel_h, mo_h, query_h,
    passage_h, qw_h, kw_h, vw_h, ao_h, blend_h,
    out_ref,
    tok, sto, gv, gg, mo, qw, kw, vw, ao, load_sem,
    ids_v, mix_gain, taps, channel_gain, query_gain, passage_gain, blend_gain, small_sem,
    ids_all, ids_s, ids_send, ids_recv, ids_sem,
    q_all, q_stage, q_send, q_recv,
    k_all, v_all, k_stage, v_stage, kv_send, kv_recv,
    gp, conv, scol, stat_all, stat_send, stat_recv, act,
    out_o, out_s, ret_o, ret_s, o_send, o_recv, s_send, s_recv,
    part, from_left, from_right, r_send, r_recv,
):
    st = lax.axis_index("st")
    tp = lax.axis_index("tp")
    core = lax.rem(st, 2)
    chip = st // 2
    n_chip = n_st // 2
    other = 1 - core
    T = tok.shape[0]
    R = sto.shape[0]
    HW = q_stage.shape[1]
    CL = act.shape[1]

    small_pairs = [(query_h, query_gain), (mix_h, mix_gain), (ids_h, ids_v), (passage_h, passage_gain),
                   (taps_h, taps), (channel_h, channel_gain), (blend_h, blend_gain)]
    big_pairs = [(tokens_h, tok), (qw_h, qw), (store_h, sto), (kw_h, kw), (vw_h, vw), (gv_h, gv), (gg_h, gg),
                 (mo_h, mo), (ao_h, ao)]
    smalls = [pltpu.make_async_copy(a, b, small_sem.at[n]) for n, (a, b) in enumerate(small_pairs)]
    loads = [pltpu.make_async_copy(a, b, load_sem.at[n]) for n, (a, b) in enumerate(big_pairs)]
    for c in smalls[:3] + loads[:2]:
        c.start()
    for c in loads[2:5] + smalls[3:] + loads[5:]:
        c.start(priority=PRIO)

    barrier = pltpu.get_barrier_semaphore()
    for i in range(1, n_st):
        pl.semaphore_signal(barrier, inc=1, device_id={"st": lax.rem(st + i, n_st)},
                            device_id_type=pl.DeviceIdType.MESH)
    for i in range(1, n_tp):
        pl.semaphore_signal(barrier, inc=1, device_id={"tp": lax.rem(tp + i, n_tp)},
                            device_id_type=pl.DeviceIdType.MESH)

    def remote(src, dst, ssem, rsem, axis, to):
        return pltpu.make_async_remote_copy(
            src_ref=src, dst_ref=dst, send_sem=ssem, recv_sem=rsem, device_id={axis: to},
            device_id_type=pl.DeviceIdType.MESH)

    chunk_rows = T // n_tp
    table = [sorted(range(n_tp), key=lambda d: -abs(d - t)) for t in range(n_tp)]

    def chunk_at(k):
        d = jnp.int32(table[0][k])
        for t in range(1, n_tp):
            d = jnp.where(tp == t, table[t][k], d)
        return d

    chunks = [chunk_at(k) for k in range(n_tp)]

    def chunk_ds(d):
        return pl.ds(pl.multiple_of(d * chunk_rows, chunk_rows), chunk_rows)

    def peers():
        res = [(chip * 2 + other, True, 0)]
        for j in range(1, n_chip):
            c = lax.rem(chip + j, n_chip)
            res.append((c * 2 + core, False, 2 * j - 1))
            res.append((c * 2 + other, True, 2 * j))
        return res

    smalls[0].wait()
    smalls[1].wait()
    loads[0].wait()
    loads[1].wait()
    TC = 256
    mine = pl.ds(pl.multiple_of(core * HW, HW), HW)
    theirs = pl.ds(pl.multiple_of(other * HW, HW), HW)

    def tok_chunk(i, carry):
        rows = pl.ds(pl.multiple_of(i * TC, TC), TC)
        x = tok[rows, :].astype(F32)
        y = x * lax.rsqrt(jnp.mean(x * x, axis=-1, keepdims=True) + EPS)
        qr = (y * query_gain[...]).astype(BF)
        q_all[st, rows, :] = mm(qr, qw[:, mine]).astype(BF)
        q_stage[rows, :] = mm(qr, qw[:, theirs]).astype(BF)
        tok[rows, :] = (y * mix_gain[...]).astype(BF)
        return carry

    lax.fori_loop(0, T // TC, tok_chunk, 0)

    pl.semaphore_wait(barrier, n_st - 1 + n_tp - 1)
    smalls[2].wait()
    for i in range(1, n_st):
        remote(ids_v, ids_all.at[st], ids_send.at[i], ids_recv.at[st], "st",
               lax.rem(st + i, n_st)).start()
    ids_own = pltpu.make_async_copy(ids_v, ids_all.at[st], ids_recv.at[st])
    ids_own.start()

    def q_copies(k):
        rows = chunk_ds(chunks[k])
        for to, stage, n in peers():
            src = q_stage.at[rows] if stage else q_all.at[st, rows]
            yield remote(src, q_all.at[st, rows], q_send.at[n, k], q_recv.at[st, k], "st", to)

    for k in range(n_tp):
        for c in q_copies(k):
            c.start()

    smalls[3].wait()
    for n in range(2, 5):
        loads[n].wait()
    RC = 512
    n_rc = R // RC
    RP = RC // pass_rows
    pass_local = R // pass_rows
    partner = chip * 2 + other

    def store_chunk(i, carry):
        rows = pl.ds(pl.multiple_of(i * RC, RC), RC)
        x = sto[rows, :].astype(F32)
        n = (x * lax.rsqrt(jnp.mean(x * x, axis=-1, keepdims=True) + EPS) * passage_gain[...]).astype(BF)
        here, slots = pl.ds(i * RP, RP), pl.ds(core * pass_local + i * RP, RP)
        k_stage[here] = mm(n, kw[:, theirs]).astype(BF).reshape(RP, pass_rows, HW)
        v_stage[here] = mm(n, vw[:, theirs]).astype(BF).reshape(RP, pass_rows, HW)
        remote(k_stage.at[here], k_all.at[slots], kv_send.at[0, i], kv_recv.at[0, i], "st", partner).start()
        remote(v_stage.at[here], v_all.at[slots], kv_send.at[1, i], kv_recv.at[1, i], "st", partner).start()
        k_all[slots] = mm(n, kw[:, mine]).astype(BF).reshape(RP, pass_rows, HW)
        v_all[slots] = mm(n, vw[:, mine]).astype(BF).reshape(RP, pass_rows, HW)
        return carry

    lax.fori_loop(0, n_rc, store_chunk, 0)

    ids_own.wait()
    for i in range(1, n_st):
        r = lax.rem(st + i, n_st)
        remote(ids_v, ids_all.at[r], ids_send.at[i], ids_recv.at[r], "st", r).wait_recv()
    c = pltpu.make_async_copy(ids_all, ids_s, ids_sem)
    c.start()
    c.wait()

    def kv_wait(i, carry):
        here, slots = pl.ds(i * RP, RP), pl.ds(other * pass_local + i * RP, RP)
        remote(k_stage.at[here], k_all.at[slots], kv_send.at[0, i], kv_recv.at[0, i], "st", partner).wait()
        remote(v_stage.at[here], v_all.at[slots], kv_send.at[1, i], kv_recv.at[1, i], "st", partner).wait()
        return carry

    lax.fori_loop(0, n_rc, kv_wait, 0)

    heads = local_heads // 2
    HD_ = HW // heads
    per_chip = 2 * pass_local
    chunk_blocks = block_count // n_tp
    clane = lax.broadcasted_iota(jnp.int32, (chunk_rows, 128), 1)
    scale = HD_ ** (-0.5)

    def order(i):
        return lax.rem(chip + 1 + i // 2, n_chip) * 2 + lax.rem(core + 1 - i % 2, 2)

    def answer_copies(k, r):
        rows = chunk_ds(chunks[k])
        return (
            remote(out_o.at[r, rows], ret_o.at[st, rows], o_send.at[r, k], o_recv.at[st, k], "st", r),
            remote(out_s.at[r, k], ret_s.at[st, k], s_send.at[r, k], s_recv.at[st, k], "st", r),
        )

    def attend(k):
        d = chunks[k]
        rows = chunk_ds(d)

        def pair(g, carry):
            rs = [order(2 * g), order(2 * g + 1)]
            for e, r in enumerate(rs):
                @pl.when(jnp.logical_or(e == 0, g < n_chip - 1))
                def _(r=r):
                    remote(q_all.at[st, rows], q_all.at[r, rows], q_send.at[0, k], q_recv.at[r, k], "st", r).wait_recv()

            units = [(e, h, u) for e in range(2) for h in range(heads) for u in range(chunk_blocks)]
            place, values, scores = {}, {}, {}
            for e, h, u in units:
                r = rs[e]
                cols = slice(h * HD_, (h + 1) * HD_)
                b = d * chunk_blocks + u
                brow = pl.ds(pl.multiple_of(b * block_len, block_len), block_len)
                ks, vs, bias = [], [], []
                for j in range(per_block):
                    p = ids_s[r, j, b] - chip * per_chip
                    spread_p = jnp.full((1, pass_rows), p, jnp.int32)
                    valid = jnp.logical_and(spread_p >= 0, spread_p < per_chip)
                    bias.append(jnp.where(valid, 0.0, NEG))
                    slot = jnp.clip(p, 0, per_chip - 1)
                    ks.append(k_all[slot][:, cols])
                    vs.append(v_all[slot][:, cols])
                s = lax.dot_general(q_all[r, brow, cols], jnp.concatenate(ks, axis=0), (((1,), (1,)), ((), ())),
                                    preferred_element_type=F32)
                scores[e, h, u] = s * scale + jnp.concatenate(bias, axis=1)
                values[e, h, u] = jnp.concatenate(vs, axis=0)
                place[e, h, u] = (r, brow, cols)
            tops = {n: jnp.maximum(jnp.max(scores[n], axis=1, keepdims=True), NEG / 2) for n in units}
            weights, dens = {}, {}
            for n in units:
                exponent = jnp.exp(scores[n] - tops[n])
                dens[n] = jnp.sum(exponent, axis=1, keepdims=True)
                weights[n] = exponent.astype(BF)
            for n in units:
                r, brow, cols = place[n]
                out_o[r, brow, cols] = mm(weights[n], values[n]).astype(BF)
            stats = jnp.zeros((chunk_rows, 128), F32)
            for e in range(2):
                for h in range(heads):
                    for at, parts in ((2 * h, tops), (2 * h + 1, dens)):
                        column = jnp.concatenate([parts[e, h, u] for u in range(chunk_blocks)], axis=0)
                        stats = jnp.where(clane == 8 * e + at, column, stats)
            turned = jnp.transpose(stats)
            for e, r in enumerate(rs):
                out_s[r, k] = turned[8 * e:8 * e + 8]

                @pl.when(jnp.logical_or(e == 0, g < n_chip - 1))
                def _(r=r):
                    for c in answer_copies(k, r):
                        c.start()

            return carry

        lax.fori_loop(0, n_chip, pair, 0)

    attend(0)

    smalls[4].wait()
    loads[5].wait()
    loads[6].wait()
    per_seq = seq_len
    pad = (gp.shape[1] - per_seq) // 2
    gp[:, :pad] = jnp.zeros((gp.shape[0], pad, CL), F32)
    gp[:, pad + per_seq:] = jnp.zeros((gp.shape[0], pad, CL), F32)

    def glu_chunk(i, carry):
        mr = tok[pl.ds(pl.multiple_of(i * TC, TC), TC), :]
        gated = (mm(mr, gv[...]) * jax.nn.sigmoid(mm(mr, gg[...]))).astype(BF).astype(F32)
        for u in range(TC // per_seq):
            gp[i * (TC // per_seq) + u, pad:pad + per_seq, :] = gated[u * per_seq:(u + 1) * per_seq]
        return carry

    lax.fori_loop(0, T // TC, glu_chunk, 0)
    tap_values = taps[...].astype(F32)
    n_tap = taps.shape[0]
    lead = pad - (n_tap - 1) // 2
    CC = 64
    per = per_seq // CC
    lane = lax.broadcasted_iota(jnp.int32, (CC, 128), 1)

    def conv_chunk(i, carry):
        seq = i // per
        base = pl.multiple_of(lax.rem(i, per) * CC, CC)
        win = gp[seq, pl.ds(base, CC + 2 * pad), :]
        acc = None
        for res in range(8):
            group = None
            for k in range(n_tap):
                if (lead + k) % 8 == res:
                    at = lead + k - res
                    term = win[at:at + CC + (8 if res else 0)] * tap_values[k:k + 1]
                    group = term if group is None else group + term
            if group is not None:
                group = group[res:res + CC]
                acc = group if acc is None else acc + group
        rows = pl.ds(pl.multiple_of(i * CC, CC), CC)
        conv[rows, :] = acc
        s = jnp.sum(acc, axis=1, keepdims=True)
        ss = jnp.sum(acc * acc, axis=1, keepdims=True)
        scol[rows, :] = jnp.where(lane == 0, s, jnp.where(lane == 1, ss, 0.0))
        return carry

    lax.fori_loop(0, T // CC, conv_chunk, 0)
    stat_all[tp] = jnp.transpose(scol[...])[:8]
    for i in range(1, n_tp):
        remote(stat_all.at[tp], stat_all.at[tp], stat_send.at[i], stat_recv.at[tp], "tp",
               lax.rem(tp + i, n_tp)).start()

    attend(1)

    smalls[5].wait()
    smalls[6].wait()
    total = stat_all[tp]
    for i in range(1, n_tp):
        r = lax.rem(tp + i, n_tp)
        remote(stat_all.at[tp], stat_all.at[r], stat_send.at[i], stat_recv.at[r], "tp", r).wait_recv()
        total = total + stat_all[r]
    ca = CL * n_tp
    mean = total / ca
    spread = jnp.transpose(jnp.concatenate([mean, jnp.zeros((120, T), F32)], axis=0))
    row_mean = spread[:, 0:1]
    inv = lax.rsqrt(spread[:, 1:2] - row_mean * row_mean + EPS)
    a = (conv[...] - row_mean) * inv * channel_gain[...]
    act[...] = (a / (1.0 + jnp.exp(-a))).astype(BF)
    loads[7].wait()
    loads[8].wait()

    SUB = 4
    SR = chunk_rows // SUB

    def hop(k, u, ahead, buf, way):
        d = chunks[k]
        prow = pl.ds(pl.multiple_of(d * chunk_rows + u * SR, SR), SR)
        brow = pl.ds(u * SR, SR)
        to = jnp.clip(tp + ahead, 0, n_tp - 1)
        return prow, brow, remote(part.at[prow], buf.at[d, brow], r_send.at[way, d, u],
                                  r_recv.at[way, d, u], "tp", to)

    ways = ((1, from_left, 0), (-1, from_right, 1))

    def goes(k, way):
        return tp < chunks[k] if way == 0 else tp > chunks[k]

    def at_end(way):
        return tp == 0 if way == 0 else tp == n_tp - 1

    def finish(k):
        rows = chunk_ds(chunks[k])
        for i in range(n_st - 1):
            r = order(i)
            remote(out_o.at[r, rows], ret_o.at[r, rows], o_send.at[r, k], o_recv.at[r, k], "st", r).wait_recv()
            remote(out_s.at[r, k], ret_s.at[r, k], s_send.at[r, k], s_recv.at[r, k], "st", r).wait_recv()
        ret_o[st, rows, :] = out_o[st, rows, :]
        ret_s[st, k] = out_s[st, k]
        stats = jnp.transpose(jnp.concatenate(
            [ret_s[c, k] for c in range(n_st)] + [jnp.zeros((128 - 8 * n_st, chunk_rows), F32)], axis=0))
        pieces = []
        for g in range(2):
            for h in range(heads):
                cols = slice(h * HD_, (h + 1) * HD_)
                at = [8 * (c * 2 + g) + 2 * h for c in range(n_chip)]
                best = functools.reduce(jnp.maximum, [stats[:, x:x + 1] for x in at])
                num, den = 0.0, 0.0
                for c in range(n_chip):
                    w = jnp.exp(stats[:, at[c]:at[c] + 1] - best)
                    num = num + w * ret_o[c * 2 + g, rows, cols].astype(F32)
                    den = den + w * stats[:, at[c] + 1:at[c] + 2]
                pieces.append((num / den).astype(BF))
        attended = jnp.concatenate(pieces, axis=1)
        act_rows = act[rows, :]
        NC = 512
        for i in range(part.shape[1] // NC):
            cols = slice(i * NC, (i + 1) * NC)
            value = mm(act_rows, mo[:, cols]) + blend_gain[:, cols] * mm(attended, ao[:, cols])
            part[rows, cols] = value.astype(BF)
        if k < n_tp - 1:
            for ahead, buf, way in ways:
                @pl.when(jnp.logical_and(goes(k, way), at_end(way)))
                def _(ahead=ahead, buf=buf, way=way):
                    for u in range(SUB):
                        hop(k, u, ahead, buf, way)[2].start()

    def forward(k, u):
        for ahead, buf, way in ways:
            @pl.when(jnp.logical_and(goes(k, way), jnp.logical_not(at_end(way))))
            def _(ahead=ahead, buf=buf, way=way):
                prow, brow, copy = hop(k, u, ahead, buf, way)
                copy.wait_recv()
                part[prow, :] = (part[prow, :].astype(F32) + buf[chunks[k], brow, :].astype(F32)).astype(BF)
                copy.start()

    forwarded = 0
    for k in range(n_tp):
        finish(k)
        if k + 2 < n_tp:
            attend(k + 2)
        elif k < n_tp - 1:
            for u in range(SUB):
                forward(k - 2, u)
            forwarded = k - 1
    for u in range(SUB):
        for k in range(forwarded, n_tp - 1):
            forward(k, u)

    for u in range(SUB):
        prow = pl.ds(pl.multiple_of(tp * chunk_rows + u * SR, SR), SR)
        brow = pl.ds(u * SR, SR)

        for ahead, buf, way in ways:
            @pl.when(jnp.logical_not(at_end(way)))
            def _(buf=buf, way=way, ahead=ahead):
                to = jnp.clip(tp - ahead, 0, n_tp - 1)
                remote(part.at[prow], buf.at[tp, brow], r_send.at[way, tp, u], r_recv.at[way, tp, u], "tp",
                       to).wait_recv()

            @pl.when(at_end(way))
            def _(buf=buf):
                buf[tp, brow, :] = jnp.zeros((SR, part.shape[1]), BF)

        out_ref[brow, :] = (
            part[prow, :].astype(F32) + from_left[tp, brow, :].astype(F32) + from_right[tp, brow, :].astype(F32)
        ).astype(BF)

    for i in range(1, n_st):
        r = lax.rem(st + i, n_st)
        remote(ids_v, ids_all.at[st], ids_send.at[i], ids_recv.at[st], "st", r).wait_send()
    for k in range(n_tp):
        for c in q_copies(k):
            c.wait_send()
        for i in range(n_st - 1):
            for c in answer_copies(k, order(i)):
                c.wait_send()
    for i in range(1, n_tp):
        remote(stat_all.at[tp], stat_all.at[tp], stat_send.at[i], stat_recv.at[tp], "tp",
               lax.rem(tp + i, n_tp)).wait_send()
    for k in range(n_tp - 1):
        for ahead, buf, way in ways:
            @pl.when(goes(k, way))
            def _(ahead=ahead, buf=buf, way=way):
                for u in range(SUB):
                    hop(k, u, ahead, buf, way)[2].wait_send()


def fused_local(
    tokens, store, passage_ids, mix_gain, glu_value, glu_gate, conv_taps, channel_gain, mix_out,
    query_gain, passage_gain, query_proj, key_proj, value_proj, attn_out, blend_gain,
):
    n_st = lax.axis_size("st")
    n_tp = lax.axis_size("tp")
    T, D = tokens.shape
    P_, PR, _ = store.shape
    R = P_ * PR
    W = query_proj.shape[1]
    HW = W // 2
    CL = glu_value.shape[1]
    nb, per_block = passage_ids.shape
    pad = 8 * pl.cdiv((conv_taps.shape[0] - 1) // 2, 8)
    DMA = pltpu.SemaphoreType.DMA
    V = pltpu.VMEM
    SUB = 4
    kern = functools.partial(layer_kernel, n_st, n_tp, nb, per_block, T // nb, W // HD, SEQ_LEN, PR)
    hbm = pl.BlockSpec(memory_space=pl.ANY)
    vm = pl.BlockSpec(memory_space=pltpu.VMEM)
    return pl.pallas_call(
        kern,
        out_shape=pltpu.VMEM((T // n_tp, D), BF),
        in_specs=[hbm] * 16,
        out_specs=vm,
        scratch_shapes=[
            V((T, D), BF), V((R, D), BF), V((D, CL), BF), V((D, CL), BF), V((CL, D), BF),
            V((D, W), BF), V((D, W), BF), V((D, W), BF), V((W, D), BF), DMA((9,)),
            V((per_block, nb), jnp.int32), V((1, D), F32), V(conv_taps.shape, BF), V((1, CL), F32), V((1, D), F32),
            V((1, D), F32), V((1, D), F32), DMA((7,)),
            V((n_st, per_block, nb), jnp.int32), pltpu.SMEM((n_st, per_block, nb), jnp.int32),
            DMA((n_st,)), DMA((n_st,)), DMA,
            V((n_st, T, HW), BF), V((T, HW), BF), DMA((n_st - 1, n_tp)), DMA((n_st, n_tp)),
            V((2 * P_, PR, HW), BF), V((2 * P_, PR, HW), BF), V((P_, PR, HW), BF), V((P_, PR, HW), BF),
            DMA((2, R // 512)), DMA((2, R // 512)),
            V((T // SEQ_LEN, SEQ_LEN + 2 * pad, CL), F32), V((T, CL), F32), V((T, 128), F32),
            V((n_tp, 8, T), F32), DMA((n_tp,)), DMA((n_tp,)), V((T, CL), BF),
            V((n_st, T, HW), BF), V((n_st, n_tp, 8, T // n_tp), F32), V((n_st, T, HW), BF),
            V((n_st, n_tp, 8, T // n_tp), F32),
            DMA((n_st, n_tp)), DMA((n_st, n_tp)), DMA((n_st, n_tp)), DMA((n_st, n_tp)),
            V((T, D), BF), V((n_tp, T // n_tp, D), BF), V((n_tp, T // n_tp, D), BF),
            DMA((2, n_tp, SUB)), DMA((2, n_tp, SUB)),
        ],
        compiler_params=pltpu.CompilerParams(
            collective_id=0, has_side_effects=True, vmem_limit_bytes=VMEM_MIB * 1024 * 1024),
        name="layer",
    )(
        tokens, store.reshape(R, D), passage_ids.T, mix_gain.reshape(1, D), glu_value, glu_gate, conv_taps,
        channel_gain.reshape(1, CL), mix_out, query_gain.reshape(1, D), passage_gain.reshape(1, D),
        query_proj, key_proj, value_proj, attn_out, blend_gain.reshape(1, D),
    )


def solution(mesh):
    in_specs = (
        P(("grp", "st"), None),
        P(("grp", "st"), None, None),
        P(("grp", "st"), None),
        P(),
        P(None, "tp"),
        P(None, "tp"),
        P(None, "tp"),
        P("tp"),
        P("tp", None),
        P(),
        P(),
        P(None, "tp"),
        P(None, "tp"),
        P(None, "tp"),
        P("tp", None),
        P(),
    )
    out_specs = P(("grp", "st", "tp"), None)
    def body(*args):
        even = args[11].shape[1] // HD % 2 == 0 and mesh.shape["st"] % 2 == 0
        even = even and args[2].shape[0] % mesh.shape["tp"] == 0 and mesh.shape["st"] <= 16
        return (fused_local if even else local)(*args)

    return jax.shard_map(body, mesh=mesh, in_specs=in_specs, out_specs=out_specs, check_vma=False)
```

```python
import functools

import jax
import jax.numpy as jnp
from jax import lax
from jax.sharding import PartitionSpec as P
from jax.experimental import pallas as pl
from jax.experimental.pallas import tpu as pltpu

CA = 1024
HD = 256
SEQ_LEN = 128


EPS = 1e-06


def rms_rows(row_data, gain_vec):
    floats = row_data.astype(jnp.float32)
    inv_scale = lax.rsqrt(jnp.mean(floats * floats, axis=-1, keepdims=True) + EPS)
    return (floats * inv_scale * gain_vec).astype(jnp.bfloat16)


def depthwise(gated_rows, conv_taps):
    span_width = conv_taps.shape[0]
    half_span = (span_width - 1) // 2
    seq_length = gated_rows.shape[1]
    padded = jnp.pad(
        gated_rows.astype(jnp.float32), ((0, 0), (half_span, span_width - 1 - half_span), (0, 0))
    )
    running = jnp.zeros(gated_rows.shape, jnp.float32)
    for tap_index in range(span_width):
        running = running + padded[:, tap_index : tap_index + seq_length] * conv_taps[
            tap_index
        ].astype(jnp.float32)
    return running


def passage_attention(queries, keys_values, head_count):
    groups, block_len, span_width = queries.shape
    head_dim = span_width // head_count
    row_count = keys_values.shape[1]
    query_heads = queries.reshape(groups, block_len, head_count, head_dim)
    key_heads = keys_values[:, :, :span_width].reshape(groups, row_count, head_count, head_dim)
    value_heads = keys_values[:, :, span_width:].reshape(groups, row_count, head_count, head_dim)
    scores = jnp.einsum(
        "gqhd,grhd->ghqr", query_heads, key_heads, preferred_element_type=jnp.float32
    ) * head_dim ** (-0.5)
    row_top = jnp.max(scores, axis=-1)
    exponent = jnp.exp(scores - row_top[..., None])
    row_sum = jnp.sum(exponent, axis=-1)
    weights = exponent.astype(jnp.bfloat16)
    outputs = jnp.einsum(
        "ghqr,grhd->gqhd", weights, value_heads, preferred_element_type=jnp.float32
    ).astype(jnp.bfloat16)
    return (outputs.reshape(groups, block_len, span_width), row_top, row_sum)


def combine(outs, tops, sums, head_count):
    batch_count, passage_count, block_len, span_width = outs.shape
    head_dim = span_width // head_count
    best_top = jnp.max(tops, axis=1, keepdims=True)
    weight = jnp.exp(tops - best_top)
    numerator = jnp.einsum(
        "bphq,bpqhd->bqhd",
        weight,
        outs.astype(jnp.float32).reshape(
            batch_count, passage_count, block_len, head_count, head_dim
        ),
    )
    denominator = jnp.sum(weight * sums, axis=1)
    result = numerator / jnp.transpose(denominator, (0, 2, 1))[..., None]
    return result.reshape(batch_count, block_len, span_width).astype(jnp.bfloat16)


def local(
    tokens,
    store,
    passage_ids,
    mix_gain,
    glu_value,
    glu_gate,
    conv_taps,
    channel_gain,
    mix_out,
    query_gain,
    passage_gain,
    query_proj,
    key_proj,
    value_proj,
    attn_out,
    blend_gain,
):
    owners = lax.axis_size("st")
    tok_rows = tokens.shape[0]
    model_width = tokens.shape[1]
    local_channels = glu_value.shape[1]
    head_width = query_proj.shape[1]
    local_heads = head_width // HD
    block_count = passage_ids.shape[0]
    per_block = passage_ids.shape[1]
    block_len = tok_rows // block_count
    requests = block_count * per_block
    capacity = 2 * requests // owners
    pass_local = store.shape[0]
    pass_rows = store.shape[1]
    flat_ids = passage_ids.reshape(requests)
    owner_of = flat_ids // pass_local
    local_of = flat_ids - owner_of * pass_local
    request_index = jnp.arange(requests)
    earlier = (owner_of[:, None] == owner_of[None, :]) & (
        request_index[None, :] < request_index[:, None]
    )
    ranking = jnp.sum(earlier.astype(jnp.int32), axis=1)
    slot_of = owner_of * capacity + ranking
    slot_ids = (
        jnp.zeros((owners * capacity,), jnp.int32)
        .at[slot_of]
        .set(local_of)
        .reshape(owners, capacity)
    )
    asked = lax.all_to_all(slot_ids, "st", split_axis=0, concat_axis=0, tiled=True)
    normed_store = rms_rows(store.reshape(pass_local * pass_rows, model_width), passage_gain)
    key_rows = jnp.dot(normed_store, key_proj, preferred_element_type=jnp.float32).astype(
        jnp.bfloat16
    )
    value_rows = jnp.dot(normed_store, value_proj, preferred_element_type=jnp.float32).astype(
        jnp.bfloat16
    )
    memory = jnp.concatenate([key_rows, value_rows], axis=1).reshape(
        pass_local, pass_rows, 2 * head_width
    )
    queries = jnp.dot(
        rms_rows(tokens, query_gain), query_proj, preferred_element_type=jnp.float32
    ).astype(jnp.bfloat16)
    query_blocks = queries.reshape(block_count, block_len, head_width)
    repeated = jnp.repeat(query_blocks, per_block, axis=0)
    served = memory[asked.reshape(owners * capacity)]
    slot_queries = (
        jnp.zeros((owners * capacity, block_len, head_width), jnp.bfloat16)
        .at[slot_of]
        .set(repeated)
    )
    visiting = lax.all_to_all(
        slot_queries.reshape(owners, capacity, block_len, head_width),
        "st",
        split_axis=0,
        concat_axis=0,
        tiled=True,
    )
    answer_out, answer_top, answer_sum = passage_attention(
        visiting.reshape(owners * capacity, block_len, head_width), served, local_heads
    )
    back_out = lax.all_to_all(
        answer_out.reshape(owners, capacity, block_len, head_width),
        "st",
        split_axis=0,
        concat_axis=0,
        tiled=True,
    )
    back_top, back_sum = (
        lax.all_to_all(
            answer_top.reshape(owners, capacity, local_heads, block_len),
            "st",
            split_axis=0,
            concat_axis=0,
            tiled=True,
        ),
        lax.all_to_all(
            answer_sum.reshape(owners, capacity, local_heads, block_len),
            "st",
            split_axis=0,
            concat_axis=0,
            tiled=True,
        ),
    )
    partial_out = back_out.reshape(owners * capacity, block_len, head_width)[slot_of]
    partial_top = back_top.reshape(owners * capacity, local_heads, block_len)[slot_of]
    partial_sum = back_sum.reshape(owners * capacity, local_heads, block_len)[slot_of]
    attended = combine(
        partial_out.reshape(block_count, per_block, block_len, head_width),
        partial_top.reshape(block_count, per_block, local_heads, block_len),
        partial_sum.reshape(block_count, per_block, local_heads, block_len),
        local_heads,
    ).reshape(tok_rows, head_width)
    mix_input = rms_rows(tokens, mix_gain)
    value_part = jnp.dot(mix_input, glu_value, preferred_element_type=jnp.float32)
    gate_part = jnp.dot(mix_input, glu_gate, preferred_element_type=jnp.float32)
    gated_rows = (value_part * jax.nn.sigmoid(gate_part)).astype(jnp.bfloat16)
    conv_rows = depthwise(gated_rows.reshape(-1, SEQ_LEN, local_channels), conv_taps).reshape(
        tok_rows, local_channels
    )
    channel_sum, channel_square = lax.psum(
        (jnp.sum(conv_rows, axis=1), jnp.sum(conv_rows * conv_rows, axis=1)), "tp"
    )
    row_mean = channel_sum / CA
    row_var = channel_square / CA - row_mean * row_mean
    activation = jax.nn.silu(
        (conv_rows - row_mean[:, None]) * lax.rsqrt(row_var + EPS)[:, None] * channel_gain
    ).astype(jnp.bfloat16)
    conv_term = jnp.dot(activation, mix_out, preferred_element_type=jnp.float32)
    attn_term = jnp.dot(attended, attn_out, preferred_element_type=jnp.float32)
    return lax.psum_scatter(
        (conv_term + blend_gain * attn_term).astype(jnp.bfloat16),
        "tp",
        scatter_dimension=0,
        tiled=True,
    )


BF = jnp.bfloat16
F32 = jnp.float32
NEG = -3e38
VMEM_MIB = 60
PRIO = 1
BEFORE = 3
RC = 512
SUB = 8
EARLY = 5


def mm(a, b):
    return jnp.dot(a, b, preferred_element_type=F32)


def wait_in(ref, sem):
    pltpu.make_async_copy(ref, ref, sem).wait()


def layer_kernel(
    n_st, n_tp, block_count, per_block, block_len, local_heads, seq_len, pass_rows,
    tokens_h, store_h, ids_h, mix_h, gv_h, gg_h, taps_h, channel_h, mo_h, query_h,
    passage_h, qw_h, kw_h, vw_h, ao_h, blend_h,
    out_ref,
    tok, sto, gv, gg, mo, qw, kw, vw, ao, load_sem,
    ids_v, mix_gain, taps, channel_gain, query_gain, passage_gain, blend_gain, small_sem,
    ids_all, ids_s, ids_send, ids_recv, ids_sem,
    q_all, q_stage, q_send, q_recv,
    k_all, v_all, k_stage, v_stage, kv_send, kv_recv,
    gp, conv, scol, stat_all, stat_send, stat_recv, act,
    out_o, out_s, ret_o, ret_s, o_send, o_recv, s_send, s_recv,
    part, inbox, r_send, r_recv,
    att, mate_act, mate_att, a_send, a_recv, mate_part, mo2, ao2, w_send, near_recv, far_recv, pass_recv,
):
    st = lax.axis_index("st")
    tp = lax.axis_index("tp")
    grp = lax.axis_index("grp")
    outer = jnp.logical_or(tp == 0, tp == n_tp - 1)
    inner = jnp.logical_not(outer)
    mate = tp + 1 - 2 * lax.rem(tp, 2)
    across = n_tp - 1 - tp
    core = lax.rem(st, 2)
    chip = st // 2
    n_chip = n_st // 2
    other = 1 - core
    T = tok.shape[0]
    R = sto.shape[0]
    HW = q_stage.shape[1]
    CL = act.shape[1]

    small_pairs = [(query_h, query_gain), (mix_h, mix_gain), (ids_h, ids_v), (passage_h, passage_gain),
                   (taps_h, taps), (channel_h, channel_gain), (blend_h, blend_gain)]
    big_pairs = [(tokens_h, tok), (qw_h, qw), (gv_h, gv), (gg_h, gg), (store_h, sto), (kw_h, kw), (vw_h, vw),
                 (mo_h, mo), (ao_h, ao)]
    smalls = [pltpu.make_async_copy(a, b, small_sem.at[n]) for n, (a, b) in enumerate(small_pairs)]
    loads = [pltpu.make_async_copy(a, b, load_sem.at[n]) for n, (a, b) in enumerate(big_pairs)]
    for c in smalls[:3] + loads[:2]:
        c.start()
    for c in loads[2:4] + smalls[3:] + loads[4:]:
        c.start(priority=PRIO)

    barrier = pltpu.get_barrier_semaphore()
    for i in range(1, n_st):
        pl.semaphore_signal(barrier, inc=1, device_id={"st": lax.rem(st + i, n_st)},
                            device_id_type=pl.DeviceIdType.MESH)
    for i in range(1, n_tp):
        pl.semaphore_signal(barrier, inc=1, device_id={"tp": lax.rem(tp + i, n_tp)},
                            device_id_type=pl.DeviceIdType.MESH)

    def remote(src, dst, ssem, rsem, axis, to):
        return pltpu.make_async_remote_copy(
            src_ref=src, dst_ref=dst, send_sem=ssem, recv_sem=rsem, device_id={axis: to},
            device_id_type=pl.DeviceIdType.MESH)

    pl.semaphore_signal(barrier, inc=1, device_id={"grp": 1 - grp}, device_id_type=pl.DeviceIdType.MESH)

    def drain(ref, sem):
        pltpu.make_async_copy(ref, ref, sem).wait()

    chunk_rows = T // n_tp
    table = [[3, 2, 1, 0], [3, 2, 0, 1], [0, 1, 3, 2], [0, 1, 2, 3]]

    def chunk_at(k):
        d = jnp.int32(table[0][k])
        for t in range(1, n_tp):
            d = jnp.where(tp == t, table[t][k], d)
        return d

    chunks = [chunk_at(k) for k in range(n_tp)]

    def chunk_ds(d):
        return pl.ds(pl.multiple_of(d * chunk_rows, chunk_rows), chunk_rows)

    def peers():
        res = [(chip * 2 + other, True, 0)]
        for j in range(1, n_chip):
            c = lax.rem(chip + j, n_chip)
            res.append((c * 2 + core, False, 2 * j - 1))
            res.append((c * 2 + other, True, 2 * j))
        return res

    partner = chip * 2 + other
    PR_ = 32
    n_ao, n_mo = HW * 2 // 4 // PR_, CL // 4 // PR_
    n_piece = n_ao + n_mo

    def weight_copy(route, p, g, c):
        src, dst, at, size = (ao_h, ao2, p, HW * 2 // 4) if p < n_ao else (mo_h, mo2, p - n_ao, CL // 4)
        rows = pl.ds(pl.multiple_of((2 * g + c) * size + at * PR_, PR_), PR_)
        axis, to = (("tp", mate), ("st", partner), ("grp", 1 - grp), ("st", partner))[route]
        arrival = (near_recv.at[p], pass_recv.at[0], far_recv.at[p], pass_recv.at[1])[route]
        return remote((dst if route else src).at[rows], dst.at[rows], w_send.at[route], arrival, axis, to)

    quarter = mo2.at[0:n_piece * PR_]

    def relay_near(*pieces):
        @pl.when(inner)
        def _():
            for p in pieces:
                weight_copy(0, p, grp, core).wait_recv()
                weight_copy(2, p, grp, core).start()
                weight_copy(1, p, grp, core).start()

    def relay_far(*pieces):
        @pl.when(inner)
        def _():
            for p in pieces:
                weight_copy(2, p, 1 - grp, core).wait_recv()
                weight_copy(3, p, 1 - grp, core).start()

    def weights_out(*pieces):
        @pl.when(outer)
        def _():
            for p in pieces:
                weight_copy(0, p, grp, core).start()

    pl.semaphore_wait(barrier, n_st - 1 + n_tp - 1 + 1)
    weights_out(*range(BEFORE))
    smalls[0].wait()
    smalls[1].wait()
    loads[0].wait()
    loads[1].wait()
    TC = 256
    mine = pl.ds(pl.multiple_of(core * HW, HW), HW)
    theirs = pl.ds(pl.multiple_of(other * HW, HW), HW)

    def tok_chunk(i, carry):
        rows = pl.ds(pl.multiple_of(i * TC, TC), TC)
        x = tok[rows, :].astype(F32)
        y = x * lax.rsqrt(jnp.mean(x * x, axis=-1, keepdims=True) + EPS)
        qr = (y * query_gain[...]).astype(BF)
        q_all[st, rows, :] = mm(qr, qw[:, mine]).astype(BF)
        q_stage[rows, :] = mm(qr, qw[:, theirs]).astype(BF)
        tok[rows, :] = (y * mix_gain[...]).astype(BF)
        return carry

    lax.fori_loop(0, T // TC, tok_chunk, 0)

    smalls[2].wait()
    for i in range(1, n_st):
        remote(ids_v, ids_all.at[st], ids_send, ids_recv, "st", lax.rem(st + i, n_st)).start()
    pltpu.make_async_copy(ids_v, ids_all.at[st], ids_recv).start()

    def q_copies(k):
        rows = chunk_ds(chunks[k])
        for to, stage, n in peers():
            src = q_stage.at[rows] if stage else q_all.at[st, rows]
            yield remote(src, q_all.at[st, rows], q_send, q_recv.at[k], "st", to)

    for k in range(n_tp):
        for c in q_copies(k):
            c.start()

    smalls[4].wait()
    loads[2].wait()
    loads[3].wait()
    per_seq = seq_len
    pad = (gp.shape[1] - per_seq) // 2
    gp[:, :pad] = jnp.zeros((gp.shape[0], pad, CL), F32)
    gp[:, pad + per_seq:] = jnp.zeros((gp.shape[0], pad, CL), F32)

    tap_values = taps[...].astype(F32)
    n_tap = taps.shape[0]
    lead = pad - (n_tap - 1) // 2
    CC = 64
    per = per_seq // CC
    lane = lax.broadcasted_iota(jnp.int32, (CC, 128), 1)

    def conv_chunk(i, carry):
        seq = i // per
        base = pl.multiple_of(lax.rem(i, per) * CC, CC)
        win = gp[seq, pl.ds(base, CC + 2 * pad), :]
        acc = None
        for res in range(8):
            group = None
            for k in range(n_tap):
                if (lead + k) % 8 == res:
                    at = lead + k - res
                    term = win[at:at + CC + (8 if res else 0)] * tap_values[k:k + 1]
                    group = term if group is None else group + term
            if group is not None:
                group = group[res:res + CC]
                acc = group if acc is None else acc + group
        rows = pl.ds(pl.multiple_of(i * CC, CC), CC)
        conv[rows, :] = acc
        s = jnp.sum(acc, axis=1, keepdims=True)
        ss = jnp.sum(acc * acc, axis=1, keepdims=True)
        scol[rows, :] = jnp.where(lane == 0, s, jnp.where(lane == 1, ss, 0.0))
        return carry

    pairs = ((0, n_tp - 1), (1, n_tp - 2))

    def glu_rows(c):
        at = c * chunk_rows
        mr = tok[at:at + chunk_rows, :]
        gated = (mm(mr, gv[...]) * jax.nn.sigmoid(mm(mr, gg[...]))).astype(BF).astype(F32)
        for u in range(chunk_rows // per_seq):
            gp[at // per_seq + u, pad:pad + per_seq, :] = gated[u * per_seq:(u + 1) * per_seq]

    def stat_copy(n, i):
        r = lax.rem(tp + i, n_tp)
        return remote(stat_all.at[tp, n], stat_all.at[tp, n], stat_send, stat_recv.at[n], "tp", r)

    def conv_pair(n):
        for c in pairs[n]:
            glu_rows(c)
        for c in pairs[n]:
            lax.fori_loop(c * chunk_rows // CC, (c + 1) * chunk_rows // CC, conv_chunk, 0)
        stat_all[tp, n] = jnp.transpose(jnp.concatenate(
            [scol[c * chunk_rows:(c + 1) * chunk_rows, :] for c in pairs[n]], axis=0))[:8]
        for i in range(1, n_tp):
            stat_copy(n, i).start()

    def act_pair(n):
        drain(stat_all.at[0:n_tp - 1, n], stat_recv.at[n])
        total = stat_all[tp, n]
        for i in range(1, n_tp):
            total = total + stat_all[lax.rem(tp + i, n_tp), n]
        mean = total / (CL * n_tp)
        spread = jnp.transpose(jnp.concatenate([mean, jnp.zeros((120, 2 * chunk_rows), F32)], axis=0))
        row_mean = spread[:, 0:1]
        inv = lax.rsqrt(spread[:, 1:2] - row_mean * row_mean + EPS)
        for j, c in enumerate(pairs[n]):
            rows, cut = slice(c * chunk_rows, (c + 1) * chunk_rows), slice(j * chunk_rows, (j + 1) * chunk_rows)
            a = (conv[rows, :] - row_mean[cut]) * inv[cut] * channel_gain[...]
            act[rows, :] = (a / (1.0 + jnp.exp(-a))).astype(BF)

    conv_pair(0)
    weights_out(*range(BEFORE, n_piece))


    drain(ids_all, ids_recv)
    ids_in = pltpu.make_async_copy(ids_all, ids_s, ids_sem)
    ids_in.start()
    smalls[3].wait()
    for n in range(4, 7):
        loads[n].wait()
    n_rc = R // RC
    RP = RC // pass_rows
    pass_local = R // pass_rows

    def norm_rows(i, part, parts):
        rows = slice(i * RC + part * RC // parts, i * RC + (part + 1) * RC // parts)
        x = sto[rows, :].astype(F32)
        y = x * lax.rsqrt(jnp.mean(x * x, axis=-1, keepdims=True) + EPS) * passage_gain[...]
        sto[rows, :] = y.astype(BF)

    for i in range(n_rc):
        norm_rows(i, 0, 1)
        here, slots = pl.ds(i * RP, RP), pl.ds(core * pass_local + i * RP, RP)
        def project(dst, at, weight, cols):
            dst[at] = mm(sto[i * RC:(i + 1) * RC, :], weight[:, cols]).astype(BF).reshape(RP, pass_rows, HW)

        project(k_stage, here, kw, theirs)
        project(v_stage, here, vw, theirs)
        remote(k_stage.at[here], k_all.at[slots], kv_send, kv_recv.at[0], "st", partner).start()
        remote(v_stage.at[here], v_all.at[slots], kv_send, kv_recv.at[1], "st", partner).start()
        relay_near(i)
        project(k_all, slots, kw, mine)
        project(v_all, slots, vw, mine)

    ids_in.wait()
    drain(k_stage, kv_recv.at[0])
    drain(v_stage, kv_recv.at[1])

    heads = local_heads // 2
    HD_ = HW // heads
    per_chip = 2 * pass_local
    chunk_blocks = block_count // n_tp
    clane = lax.broadcasted_iota(jnp.int32, (chunk_rows, 128), 1)
    scale = HD_ ** (-0.5)

    def order(i):
        return lax.rem(chip + 1 + i // 2, n_chip) * 2 + lax.rem(core + 1 - i % 2, 2)

    def answer_copies(k, r):
        rows = chunk_ds(chunks[k])
        return (
            remote(out_o.at[r, rows], ret_o.at[st, rows], o_send, o_recv.at[k], "st", r),
            remote(out_s.at[r, k], ret_s.at[st, k], s_send, s_recv.at[k], "st", r),
        )

    def attend(k):
        d = chunks[k]
        rows = chunk_ds(d)

        rs = [order(i) for i in range(n_st)]
        drain(q_all.at[0:n_st - 1, rows], q_recv.at[k])
        units = [(e, h, u) for e in range(n_st) for h in range(heads) for u in range(chunk_blocks)]
        place, values, scores, tops, dens, weights = {}, {}, {}, {}, {}, {}
        for e, h, u in units:
            r = rs[e]
            cols = slice(h * HD_, (h + 1) * HD_)
            b = d * chunk_blocks + u
            brow = pl.ds(pl.multiple_of(b * block_len, block_len), block_len)
            ks, vs, bias = [], [], []
            for j in range(per_block):
                p = ids_s[r, j, b] - chip * per_chip
                spread_p = jnp.full((1, pass_rows), p, jnp.int32)
                valid = jnp.logical_and(spread_p >= 0, spread_p < per_chip)
                bias.append(jnp.where(valid, 0.0, NEG))
                slot = jnp.clip(p, 0, per_chip - 1)
                ks.append(k_all[slot][:, cols])
                vs.append(functools.partial(lambda slot, cols: v_all[slot][:, cols], slot, cols))
            s = lax.dot_general(q_all[r, brow, cols], jnp.concatenate(ks, axis=0), (((1,), (1,)), ((), ())),
                                preferred_element_type=F32)
            scores[e, h, u] = s * scale + jnp.concatenate(bias, axis=1)
            values[e, h, u] = vs
            place[e, h, u] = (r, brow, cols)
        for e0 in range(0, n_st, 2):
            batch = [n for n in units if n[0] in (e0, e0 + 1)]
            for n in batch:
                tops[n] = jnp.maximum(jnp.max(scores[n], axis=1, keepdims=True), NEG / 2)
            for n in batch:
                exponent = jnp.exp(scores[n] - tops[n])
                dens[n] = jnp.sum(exponent, axis=1, keepdims=True)
                weights[n] = exponent.astype(BF)
            for n in batch:
                r, brow, cols = place[n]
                out_o[r, brow, cols] = mm(weights[n], jnp.concatenate([v() for v in values[n]], axis=0)).astype(BF)
            stats = jnp.zeros((chunk_rows, 128), F32)
            for e in range(2):
                for h in range(heads):
                    for at, parts in ((2 * h, tops), (2 * h + 1, dens)):
                        column = jnp.concatenate([parts[e0 + e, h, u] for u in range(chunk_blocks)], axis=0)
                        stats = jnp.where(clane == 8 * e + at, column, stats)
            turned = jnp.transpose(stats)
            for e in range(2):
                r = rs[e0 + e]
                out_s[r, k] = turned[8 * e:8 * e + 8]
                if e0 + e < n_st - 1:
                    for c in answer_copies(k, r):
                        c.start()

    attend(0)
    relay_near(2)
    conv_pair(1)
    relay_near(3)
    relay_far(0)
    attend(1)
    relay_far(1)
    attend(2)
    relay_near(4)
    relay_far(2)
    smalls[5].wait()
    smalls[6].wait()
    act_pair(0)
    loads[7].wait()
    loads[8].wait()

    SR = chunk_rows // SUB
    AH = chunk_rows // 2
    NC = 512

    def piece(lane, u):
        d = chunks[(0, 0, 1, 2)[lane]]
        rows = pl.ds(pl.multiple_of(d * chunk_rows + u * SR, SR), SR)
        slot = (0, 1, 2, 0)[lane]
        to = (mate, across, across, mate)[lane]
        box = inbox.at[slot, pl.ds(u * SR, SR)]
        return rows, slot, remote(part.at[rows], box, r_send, r_recv.at[slot, u], "tp", to)

    def rows_copies(k, half):
        rows = pl.ds(pl.multiple_of(chunks[k] * chunk_rows + half * AH, AH), AH)
        cut = pl.ds(half * AH, AH)
        return (
            remote(act.at[rows], mate_act.at[k - 1, cut], a_send.at[0], a_recv.at[0, k - 1, half], "tp", mate),
            remote(att.at[k, cut], mate_att.at[k - 1, cut], a_send.at[1], a_recv.at[1, k - 1, half], "tp", mate),
        )

    def combine(k):
        rows = chunk_ds(chunks[k])
        drain(ret_o.at[0:n_st - 1, rows], o_recv.at[k])
        drain(ret_s.at[0:n_st - 1, k], s_recv.at[k])
        ret_s[st, k] = out_s[st, k]
        stats = jnp.transpose(jnp.concatenate(
            [ret_s[c, k] for c in range(n_st)] + [jnp.zeros((128 - 8 * n_st, chunk_rows), F32)], axis=0))
        ret_o[st, rows, :] = out_o[st, rows, :]
        for g in range(2):
            for h in range(heads):
                cols = slice(h * HD_, (h + 1) * HD_)
                at = [8 * (c * 2 + g) + 2 * h for c in range(n_chip)]
                best = functools.reduce(jnp.maximum, [stats[:, x:x + 1] for x in at])
                num, den = 0.0, 0.0
                for c in range(n_chip):
                    w = jnp.exp(stats[:, at[c]:at[c] + 1] - best)
                    num = num + w * ret_o[c * 2 + g, rows, cols].astype(F32)
                    den = den + w * stats[:, at[c] + 1:at[c] + 2]
                att[k, :, (g * heads + h) * HD_:(g * heads + h + 1) * HD_] = (num / den).astype(BF)

    def own_partial(k):
        rows = chunk_ds(chunks[k])
        for i in range(part.shape[1] // NC):
            cols = slice(i * NC, (i + 1) * NC)
            part[rows, cols] = (mm(act[rows, :], mo[:, cols]) + blend_gain[:, cols] * mm(att[k], ao[:, cols])).astype(BF)

    def mate_rows(slot, half, cols):
        cut = slice(half * AH, (half + 1) * AH)
        return (mm(mate_act[slot, cut], mo2[:, cols])
                + blend_gain[:, cols] * mm(mate_att[slot, cut], ao2[:, cols])).astype(BF)

    def wait_rows(k, half):
        for c in rows_copies(k, half):
            c.wait_recv()

    def onward(lane_in, lane_out, *pieces):
        for u in pieces:
            slot = (0, 1, 2, 0)[lane_in]
            piece(lane_in, u)[2].wait_recv()
            rows, _, copy = piece(lane_out, u)
            part[rows, :] = (part[rows, :].astype(F32) + inbox[slot, pl.ds(u * SR, SR), :].astype(F32)).astype(BF)
            copy.start()

    combine(0)
    own_partial(0)

    @pl.when(outer)
    def _():
        for u in range(EARLY):
            piece(0, u)[2].start()

    relay_near(5)
    relay_far(3)
    act_pair(1)
    attend(3)
    combine(1)

    @pl.when(outer)
    def _():
        for half in range(2):
            for c in rows_copies(1, half):
                c.start()
        for u in range(EARLY, SUB):
            piece(0, u)[2].start()

    @pl.when(inner)
    def _():
        onward(0, 1, 0)
        own_partial(1)
        onward(0, 1, 1)

    combine(2)

    @pl.when(outer)
    def _():
        for half in range(2):
            for c in rows_copies(2, half):
                c.start()

    relay_far(4, 5)

    @pl.when(inner)
    def _():
        onward(0, 1, *range(2, EARLY))
        own_partial(2)

    combine(3)
    own_partial(3)

    @pl.when(inner)
    def _():
        for n in range(2):
            drain(quarter, pass_recv.at[n])
        for half in range(2):
            wait_rows(1, half)
            rows = pl.ds(pl.multiple_of(chunks[1] * chunk_rows + half * AH, AH), AH)
            for i in range(part.shape[1] // NC):
                cols = slice(i * NC, (i + 1) * NC)
                part[rows, cols] = (part[rows, cols].astype(F32) + mate_rows(0, half, cols).astype(F32)).astype(BF)
            for u in range(half * SUB // 2, (half + 1) * SUB // 2):
                piece(2, u)[2].start()
            if half == 0:
                onward(0, 1, *range(EARLY, SUB))
        onward(1, 3, *range(EARLY))
        for half in range(2):
            wait_rows(2, half)
            for i in range(part.shape[1] // NC):
                cols = slice(i * NC, (i + 1) * NC)
                mate_part[half * AH:(half + 1) * AH, cols] = mate_rows(1, half, cols)
        onward(1, 3, *range(EARLY, SUB))
        for u in range(SUB):
            rows = pl.ds(pl.multiple_of(tp * chunk_rows + u * SR, SR), SR)
            cut = pl.ds(u * SR, SR)
            piece(2, u)[2].wait_recv()
            out_ref[cut, :] = (part[rows, :].astype(F32) + mate_part[cut, :].astype(F32)
                               + inbox[2, cut, :].astype(F32)).astype(BF)

    @pl.when(outer)
    def _():
        for u in range(SUB):
            rows = pl.ds(pl.multiple_of(tp * chunk_rows + u * SR, SR), SR)
            cut = pl.ds(u * SR, SR)
            piece(3, u)[2].wait_recv()
            out_ref[cut, :] = (part[rows, :].astype(F32) + inbox[0, cut, :].astype(F32)).astype(BF)

    @pl.when(outer)
    def _():
        drain(quarter, w_send.at[0])
        drain(part.at[0:chunk_rows], r_send)
        drain(act.at[0:2 * chunk_rows], a_send.at[0])
        drain(att.at[0:2], a_send.at[1])

    @pl.when(inner)
    def _():
        for route in (1, 2, 3):
            drain(quarter, w_send.at[route])
        drain(part.at[0:3 * chunk_rows], r_send)

    drain(ids_all.at[0:n_st - 1], ids_send)
    drain(q_all.at[0:n_st - 1], q_send)
    drain(k_all, kv_send)
    drain(stat_all.at[0:n_tp - 1], stat_send)
    drain(out_o.at[0:n_st - 1], o_send)
    drain(out_s.at[0:n_st - 1], s_send)


def fused_local(
    tokens, store, passage_ids, mix_gain, glu_value, glu_gate, conv_taps, channel_gain, mix_out,
    query_gain, passage_gain, query_proj, key_proj, value_proj, attn_out, blend_gain,
):
    n_st = lax.axis_size("st")
    n_tp = lax.axis_size("tp")
    T, D = tokens.shape
    P_, PR, _ = store.shape
    R = P_ * PR
    W = query_proj.shape[1]
    HW = W // 2
    CL = glu_value.shape[1]
    nb, per_block = passage_ids.shape
    pad = 8 * pl.cdiv((conv_taps.shape[0] - 1) // 2, 8)
    DMA = pltpu.SemaphoreType.DMA
    V = pltpu.VMEM
    kern = functools.partial(layer_kernel, n_st, n_tp, nb, per_block, T // nb, W // HD, SEQ_LEN, PR)
    hbm = pl.BlockSpec(memory_space=pl.ANY)
    vm = pl.BlockSpec(memory_space=pltpu.VMEM)
    return pl.pallas_call(
        kern,
        out_shape=pltpu.VMEM((T // n_tp, D), BF),
        in_specs=[hbm] * 16,
        out_specs=vm,
        scratch_shapes=[
            V((T, D), BF), V((R, D), BF), V((D, CL), BF), V((D, CL), BF), V((CL, D), BF),
            V((D, W), BF), V((D, W), BF), V((D, W), BF), V((W, D), BF), DMA((9,)),
            V((per_block, nb), jnp.int32), V((1, D), F32), V(conv_taps.shape, BF), V((1, CL), F32), V((1, D), F32),
            V((1, D), F32), V((1, D), F32), DMA((7,)),
            V((n_st, per_block, nb), jnp.int32), pltpu.SMEM((n_st, per_block, nb), jnp.int32),
            DMA, DMA, DMA,
            V((n_st, T, HW), BF), V((T, HW), BF), DMA, DMA((n_tp,)),
            V((2 * P_, PR, HW), BF), V((2 * P_, PR, HW), BF), V((P_, PR, HW), BF), V((P_, PR, HW), BF),
            DMA, DMA((2,)),
            V((T // SEQ_LEN, SEQ_LEN + 2 * pad, CL), F32), V((T, CL), F32), V((T, 128), F32),
            V((n_tp, 2, 8, 2 * T // n_tp), F32), DMA, DMA((2,)), V((T, CL), BF),
            V((n_st, T, HW), BF), V((n_st, n_tp, 8, T // n_tp), F32), V((n_st, T, HW), BF),
            V((n_st, n_tp, 8, T // n_tp), F32),
            DMA, DMA((n_tp,)), DMA, DMA((n_tp,)),
            V((T, D), BF), V((3, T // n_tp, D), BF), DMA, DMA((3, SUB)),
            V((n_tp, T // n_tp, W), BF), V((2, T // n_tp, CL), BF), V((2, T // n_tp, W), BF),
            DMA((2,)), DMA((2, 2, 2)), V((T // n_tp, D), BF), V((CL, D), BF), V((W, D), BF),
            DMA((4,)), DMA(((W + CL) // 128,)), DMA(((W + CL) // 128,)), DMA((2,)),
        ],
        compiler_params=pltpu.CompilerParams(
            collective_id=0, has_side_effects=True, vmem_limit_bytes=VMEM_MIB * 1024 * 1024),
        name="layer",
    )(
        tokens, store.reshape(R, D), passage_ids.T, mix_gain.reshape(1, D), glu_value, glu_gate, conv_taps,
        channel_gain.reshape(1, CL), mix_out, query_gain.reshape(1, D), passage_gain.reshape(1, D),
        query_proj, key_proj, value_proj, attn_out, blend_gain.reshape(1, D),
    )


def solution(mesh):
    in_specs = (
        P(("grp", "st"), None),
        P(("grp", "st"), None, None),
        P(("grp", "st"), None),
        P(),
        P(None, "tp"),
        P(None, "tp"),
        P(None, "tp"),
        P("tp"),
        P("tp", None),
        P(),
        P(),
        P(None, "tp"),
        P(None, "tp"),
        P(None, "tp"),
        P("tp", None),
        P(),
    )
    out_specs = P(("grp", "st", "tp"), None)
    def body(*args):
        even = args[11].shape[1] // HD % 2 == 0 and mesh.shape["st"] % 2 == 0
        even = even and args[2].shape[0] % mesh.shape["tp"] == 0 and mesh.shape["st"] <= 16
        even = even and mesh.shape["tp"] == 4 and mesh.shape["grp"] == 2 and mesh.shape["st"] == 4
        even = even and args[0].shape[0] % (SEQ_LEN * mesh.shape["tp"]) == 0
        return (fused_local if even else local)(*args)

    return jax.shard_map(body, mesh=mesh, in_specs=in_specs, out_specs=out_specs, check_vma=False)
```

```python
import functools

import jax
import jax.numpy as jnp
from jax import lax
from jax.sharding import PartitionSpec as P
from jax.experimental import pallas as pl
from jax.experimental.pallas import tpu as pltpu

CA = 1024
HD = 256
SEQ_LEN = 128


EPS = 1e-06


def rms_rows(row_data, gain_vec):
    floats = row_data.astype(jnp.float32)
    inv_scale = lax.rsqrt(jnp.mean(floats * floats, axis=-1, keepdims=True) + EPS)
    return (floats * inv_scale * gain_vec).astype(jnp.bfloat16)


def depthwise(gated_rows, conv_taps):
    span_width = conv_taps.shape[0]
    half_span = (span_width - 1) // 2
    seq_length = gated_rows.shape[1]
    padded = jnp.pad(
        gated_rows.astype(jnp.float32), ((0, 0), (half_span, span_width - 1 - half_span), (0, 0))
    )
    running = jnp.zeros(gated_rows.shape, jnp.float32)
    for tap_index in range(span_width):
        running = running + padded[:, tap_index : tap_index + seq_length] * conv_taps[
            tap_index
        ].astype(jnp.float32)
    return running


def passage_attention(queries, keys_values, head_count):
    groups, block_len, span_width = queries.shape
    head_dim = span_width // head_count
    row_count = keys_values.shape[1]
    query_heads = queries.reshape(groups, block_len, head_count, head_dim)
    key_heads = keys_values[:, :, :span_width].reshape(groups, row_count, head_count, head_dim)
    value_heads = keys_values[:, :, span_width:].reshape(groups, row_count, head_count, head_dim)
    scores = jnp.einsum(
        "gqhd,grhd->ghqr", query_heads, key_heads, preferred_element_type=jnp.float32
    ) * head_dim ** (-0.5)
    row_top = jnp.max(scores, axis=-1)
    exponent = jnp.exp(scores - row_top[..., None])
    row_sum = jnp.sum(exponent, axis=-1)
    weights = exponent.astype(jnp.bfloat16)
    outputs = jnp.einsum(
        "ghqr,grhd->gqhd", weights, value_heads, preferred_element_type=jnp.float32
    ).astype(jnp.bfloat16)
    return (outputs.reshape(groups, block_len, span_width), row_top, row_sum)


def combine(outs, tops, sums, head_count):
    batch_count, passage_count, block_len, span_width = outs.shape
    head_dim = span_width // head_count
    best_top = jnp.max(tops, axis=1, keepdims=True)
    weight = jnp.exp(tops - best_top)
    numerator = jnp.einsum(
        "bphq,bpqhd->bqhd",
        weight,
        outs.astype(jnp.float32).reshape(
            batch_count, passage_count, block_len, head_count, head_dim
        ),
    )
    denominator = jnp.sum(weight * sums, axis=1)
    result = numerator / jnp.transpose(denominator, (0, 2, 1))[..., None]
    return result.reshape(batch_count, block_len, span_width).astype(jnp.bfloat16)


def local(
    tokens,
    store,
    passage_ids,
    mix_gain,
    glu_value,
    glu_gate,
    conv_taps,
    channel_gain,
    mix_out,
    query_gain,
    passage_gain,
    query_proj,
    key_proj,
    value_proj,
    attn_out,
    blend_gain,
):
    owners = lax.axis_size("st")
    tok_rows = tokens.shape[0]
    model_width = tokens.shape[1]
    local_channels = glu_value.shape[1]
    head_width = query_proj.shape[1]
    local_heads = head_width // HD
    block_count = passage_ids.shape[0]
    per_block = passage_ids.shape[1]
    block_len = tok_rows // block_count
    requests = block_count * per_block
    capacity = 2 * requests // owners
    pass_local = store.shape[0]
    pass_rows = store.shape[1]
    flat_ids = passage_ids.reshape(requests)
    owner_of = flat_ids // pass_local
    local_of = flat_ids - owner_of * pass_local
    request_index = jnp.arange(requests)
    earlier = (owner_of[:, None] == owner_of[None, :]) & (
        request_index[None, :] < request_index[:, None]
    )
    ranking = jnp.sum(earlier.astype(jnp.int32), axis=1)
    slot_of = owner_of * capacity + ranking
    slot_ids = (
        jnp.zeros((owners * capacity,), jnp.int32)
        .at[slot_of]
        .set(local_of)
        .reshape(owners, capacity)
    )
    asked = lax.all_to_all(slot_ids, "st", split_axis=0, concat_axis=0, tiled=True)
    normed_store = rms_rows(store.reshape(pass_local * pass_rows, model_width), passage_gain)
    key_rows = jnp.dot(normed_store, key_proj, preferred_element_type=jnp.float32).astype(
        jnp.bfloat16
    )
    value_rows = jnp.dot(normed_store, value_proj, preferred_element_type=jnp.float32).astype(
        jnp.bfloat16
    )
    memory = jnp.concatenate([key_rows, value_rows], axis=1).reshape(
        pass_local, pass_rows, 2 * head_width
    )
    queries = jnp.dot(
        rms_rows(tokens, query_gain), query_proj, preferred_element_type=jnp.float32
    ).astype(jnp.bfloat16)
    query_blocks = queries.reshape(block_count, block_len, head_width)
    repeated = jnp.repeat(query_blocks, per_block, axis=0)
    served = memory[asked.reshape(owners * capacity)]
    slot_queries = (
        jnp.zeros((owners * capacity, block_len, head_width), jnp.bfloat16)
        .at[slot_of]
        .set(repeated)
    )
    visiting = lax.all_to_all(
        slot_queries.reshape(owners, capacity, block_len, head_width),
        "st",
        split_axis=0,
        concat_axis=0,
        tiled=True,
    )
    answer_out, answer_top, answer_sum = passage_attention(
        visiting.reshape(owners * capacity, block_len, head_width), served, local_heads
    )
    back_out = lax.all_to_all(
        answer_out.reshape(owners, capacity, block_len, head_width),
        "st",
        split_axis=0,
        concat_axis=0,
        tiled=True,
    )
    back_top, back_sum = (
        lax.all_to_all(
            answer_top.reshape(owners, capacity, local_heads, block_len),
            "st",
            split_axis=0,
            concat_axis=0,
            tiled=True,
        ),
        lax.all_to_all(
            answer_sum.reshape(owners, capacity, local_heads, block_len),
            "st",
            split_axis=0,
            concat_axis=0,
            tiled=True,
        ),
    )
    partial_out = back_out.reshape(owners * capacity, block_len, head_width)[slot_of]
    partial_top = back_top.reshape(owners * capacity, local_heads, block_len)[slot_of]
    partial_sum = back_sum.reshape(owners * capacity, local_heads, block_len)[slot_of]
    attended = combine(
        partial_out.reshape(block_count, per_block, block_len, head_width),
        partial_top.reshape(block_count, per_block, local_heads, block_len),
        partial_sum.reshape(block_count, per_block, local_heads, block_len),
        local_heads,
    ).reshape(tok_rows, head_width)
    mix_input = rms_rows(tokens, mix_gain)
    value_part = jnp.dot(mix_input, glu_value, preferred_element_type=jnp.float32)
    gate_part = jnp.dot(mix_input, glu_gate, preferred_element_type=jnp.float32)
    gated_rows = (value_part * jax.nn.sigmoid(gate_part)).astype(jnp.bfloat16)
    conv_rows = depthwise(gated_rows.reshape(-1, SEQ_LEN, local_channels), conv_taps).reshape(
        tok_rows, local_channels
    )
    channel_sum, channel_square = lax.psum(
        (jnp.sum(conv_rows, axis=1), jnp.sum(conv_rows * conv_rows, axis=1)), "tp"
    )
    row_mean = channel_sum / CA
    row_var = channel_square / CA - row_mean * row_mean
    activation = jax.nn.silu(
        (conv_rows - row_mean[:, None]) * lax.rsqrt(row_var + EPS)[:, None] * channel_gain
    ).astype(jnp.bfloat16)
    conv_term = jnp.dot(activation, mix_out, preferred_element_type=jnp.float32)
    attn_term = jnp.dot(attended, attn_out, preferred_element_type=jnp.float32)
    return lax.psum_scatter(
        (conv_term + blend_gain * attn_term).astype(jnp.bfloat16),
        "tp",
        scatter_dimension=0,
        tiled=True,
    )


BF = jnp.bfloat16
F32 = jnp.float32
NEG = -3e38
VMEM_MIB = 60
PRIO = 1
BEFORE = 3
RC = 512
SUB = 8
EARLY = 5
LATE = 4


def mm(a, b):
    return jnp.dot(a, b, preferred_element_type=F32)


def wait_in(ref, sem):
    pltpu.make_async_copy(ref, ref, sem).wait()


def layer_kernel(
    n_st, n_tp, block_count, per_block, block_len, local_heads, seq_len, pass_rows,
    tokens_h, store_h, ids_h, mix_h, gv_h, gg_h, taps_h, channel_h, mo_h, query_h,
    passage_h, qw_h, kw_h, vw_h, ao_h, blend_h,
    out_ref,
    tok, sto, gv, gg, mo, qw, kw, vw, ao, load_sem,
    ids_v, mix_gain, taps, channel_gain, query_gain, passage_gain, blend_gain, small_sem,
    ids_all, ids_s, ids_send, ids_recv, ids_sem,
    q_all, q_stage, q_send, q_recv,
    k_all, v_all, k_stage, v_stage, kv_send, kv_recv,
    gp, conv, scol, stat_all, stat_send, stat_recv, act,
    out_o, out_s, ret_o, ret_s, o_send, o_recv, s_send, s_recv,
    part, inbox, r_send, r_recv,
    att, mate_act, mate_att, a_send, a_recv, mate_part, mo2, ao2, w_send, near_recv, far_recv, pass_recv,
):
    st = lax.axis_index("st")
    tp = lax.axis_index("tp")
    grp = lax.axis_index("grp")
    outer = jnp.logical_or(tp == 0, tp == n_tp - 1)
    inner = jnp.logical_not(outer)
    mate = tp + 1 - 2 * lax.rem(tp, 2)
    across = n_tp - 1 - tp
    core = lax.rem(st, 2)
    chip = st // 2
    n_chip = n_st // 2
    other = 1 - core
    T = tok.shape[0]
    R = sto.shape[0]
    HW = q_stage.shape[1]
    CL = act.shape[1]

    small_pairs = [(query_h, query_gain), (mix_h, mix_gain), (ids_h, ids_v), (passage_h, passage_gain),
                   (taps_h, taps), (channel_h, channel_gain), (blend_h, blend_gain)]
    big_pairs = [(tokens_h, tok), (qw_h, qw), (gv_h, gv), (gg_h, gg), (store_h, sto), (kw_h, kw), (vw_h, vw),
                 (mo_h, mo), (ao_h, ao)]
    smalls = [pltpu.make_async_copy(a, b, small_sem.at[n]) for n, (a, b) in enumerate(small_pairs)]
    loads = [pltpu.make_async_copy(a, b, load_sem.at[n]) for n, (a, b) in enumerate(big_pairs)]
    for c in smalls[:3] + loads[:2]:
        c.start()
    for c in loads[2:4] + smalls[3:] + loads[4:]:
        c.start(priority=PRIO)

    barrier = pltpu.get_barrier_semaphore()
    for i in range(1, n_st):
        pl.semaphore_signal(barrier, inc=1, device_id={"st": lax.rem(st + i, n_st)},
                            device_id_type=pl.DeviceIdType.MESH)
    for i in range(1, n_tp):
        pl.semaphore_signal(barrier, inc=1, device_id={"tp": lax.rem(tp + i, n_tp)},
                            device_id_type=pl.DeviceIdType.MESH)

    def remote(src, dst, ssem, rsem, axis, to):
        return pltpu.make_async_remote_copy(
            src_ref=src, dst_ref=dst, send_sem=ssem, recv_sem=rsem, device_id={axis: to},
            device_id_type=pl.DeviceIdType.MESH)

    pl.semaphore_signal(barrier, inc=1, device_id={"grp": 1 - grp}, device_id_type=pl.DeviceIdType.MESH)

    def drain(ref, sem):
        pltpu.make_async_copy(ref, ref, sem).wait()

    chunk_rows = T // n_tp
    table = [[3, 2, 1, 0], [3, 2, 0, 1], [0, 1, 3, 2], [0, 1, 2, 3]]

    def chunk_at(k):
        d = jnp.int32(table[0][k])
        for t in range(1, n_tp):
            d = jnp.where(tp == t, table[t][k], d)
        return d

    chunks = [chunk_at(k) for k in range(n_tp)]

    def chunk_ds(d):
        return pl.ds(pl.multiple_of(d * chunk_rows, chunk_rows), chunk_rows)

    def peers():
        res = [(chip * 2 + other, True, 0)]
        for j in range(1, n_chip):
            c = lax.rem(chip + j, n_chip)
            res.append((c * 2 + core, False, 2 * j - 1))
            res.append((c * 2 + other, True, 2 * j))
        return res

    partner = chip * 2 + other
    PR_ = 32
    n_ao, n_mo = HW * 2 // 4 // PR_, CL // 4 // PR_
    n_piece = n_ao + n_mo

    def weight_copy(route, p, g, c):
        src, dst, at, size = (ao_h, ao2, p, HW * 2 // 4) if p < n_ao else (mo_h, mo2, p - n_ao, CL // 4)
        rows = pl.ds(pl.multiple_of((2 * g + c) * size + at * PR_, PR_), PR_)
        axis, to = (("tp", mate), ("st", partner), ("grp", 1 - grp), ("st", partner))[route]
        arrival = (near_recv.at[p], pass_recv.at[0], far_recv.at[p], pass_recv.at[1])[route]
        return remote((dst if route else src).at[rows], dst.at[rows], w_send.at[route], arrival, axis, to)

    quarter = mo2.at[0:n_piece * PR_]

    def relay_near(*steps):
        @pl.when(inner)
        def _():
            for p in steps:
                weight_copy(0, p, grp, core).wait_recv()
                weight_copy(2, p, grp, core).start()
                weight_copy(1, p, grp, core).start()

    def relay_far(*steps):
        @pl.when(inner)
        def _():
            for p in steps:
                weight_copy(2, p, 1 - grp, core).wait_recv()
                weight_copy(3, p, 1 - grp, core).start()

    def weights_out(*steps):
        @pl.when(outer)
        def _():
            for p in steps:
                weight_copy(0, p, grp, core).start()

    pl.semaphore_wait(barrier, n_st - 1 + n_tp - 1 + 1)
    weights_out(*range(BEFORE))
    smalls[0].wait()
    smalls[1].wait()
    loads[0].wait()
    loads[1].wait()
    TC = 256
    mine = pl.ds(pl.multiple_of(core * HW, HW), HW)
    theirs = pl.ds(pl.multiple_of(other * HW, HW), HW)

    def tok_chunk(i, carry):
        rows = pl.ds(pl.multiple_of(i * TC, TC), TC)
        x = tok[rows, :].astype(F32)
        y = x * lax.rsqrt(jnp.mean(x * x, axis=-1, keepdims=True) + EPS)
        qr = (y * query_gain[...]).astype(BF)
        q_all[st, rows, :] = mm(qr, qw[:, mine]).astype(BF)
        q_stage[rows, :] = mm(qr, qw[:, theirs]).astype(BF)
        tok[rows, :] = (y * mix_gain[...]).astype(BF)
        return carry

    lax.fori_loop(0, T // TC, tok_chunk, 0)

    smalls[2].wait()
    for i in range(1, n_st):
        remote(ids_v, ids_all.at[st], ids_send, ids_recv, "st", lax.rem(st + i, n_st)).start()
    pltpu.make_async_copy(ids_v, ids_all.at[st], ids_recv).start()

    def q_copies(k):
        rows = chunk_ds(chunks[k])
        for to, stage, n in peers():
            src = q_stage.at[rows] if stage else q_all.at[st, rows]
            yield remote(src, q_all.at[st, rows], q_send, q_recv.at[k], "st", to)

    for k in range(n_tp - 1):
        for c in q_copies(k):
            c.start()

    smalls[4].wait()
    loads[2].wait()
    loads[3].wait()
    per_seq = seq_len
    pad = (gp.shape[1] - per_seq) // 2
    gp[:, :pad] = jnp.zeros((gp.shape[0], pad, CL), F32)
    gp[:, pad + per_seq:] = jnp.zeros((gp.shape[0], pad, CL), F32)

    tap_values = taps[...].astype(F32)
    n_tap = taps.shape[0]
    lead = pad - (n_tap - 1) // 2
    CC = 64
    per = per_seq // CC
    lane = lax.broadcasted_iota(jnp.int32, (CC, 128), 1)

    def conv_chunk(i, carry):
        seq = i // per
        base = pl.multiple_of(lax.rem(i, per) * CC, CC)
        win = gp[seq, pl.ds(base, CC + 2 * pad), :]
        acc = None
        for res in range(8):
            group = None
            for k in range(n_tap):
                if (lead + k) % 8 == res:
                    at = lead + k - res
                    term = win[at:at + CC + (8 if res else 0)] * tap_values[k:k + 1]
                    group = term if group is None else group + term
            if group is not None:
                group = group[res:res + CC]
                acc = group if acc is None else acc + group
        rows = pl.ds(pl.multiple_of(i * CC, CC), CC)
        conv[rows, :] = acc
        s = jnp.sum(acc, axis=1, keepdims=True)
        ss = jnp.sum(acc * acc, axis=1, keepdims=True)
        scol[rows, :] = jnp.where(lane == 0, s, jnp.where(lane == 1, ss, 0.0))
        return carry

    pairs = ((0, n_tp - 1), (1, n_tp - 2))

    def glu_rows(c):
        at = c * chunk_rows
        mr = tok[at:at + chunk_rows, :]
        gated = (mm(mr, gv[...]) * jax.nn.sigmoid(mm(mr, gg[...]))).astype(BF).astype(F32)
        for u in range(chunk_rows // per_seq):
            gp[at // per_seq + u, pad:pad + per_seq, :] = gated[u * per_seq:(u + 1) * per_seq]

    def stat_copy(n, i):
        r = lax.rem(tp + i, n_tp)
        return remote(stat_all.at[tp, n], stat_all.at[tp, n], stat_send, stat_recv.at[n], "tp", r)

    def conv_pair(n):
        for c in pairs[n]:
            glu_rows(c)
        for c in pairs[n]:
            lax.fori_loop(c * chunk_rows // CC, (c + 1) * chunk_rows // CC, conv_chunk, 0)
        stat_all[tp, n] = jnp.transpose(jnp.concatenate(
            [scol[c * chunk_rows:(c + 1) * chunk_rows, :] for c in pairs[n]], axis=0))[:8]
        for i in range(1, n_tp):
            stat_copy(n, i).start()

    def act_pair(n):
        drain(stat_all.at[0:n_tp - 1, n], stat_recv.at[n])
        total = stat_all[tp, n]
        for i in range(1, n_tp):
            total = total + stat_all[lax.rem(tp + i, n_tp), n]
        mean = total / (CL * n_tp)
        spread = jnp.transpose(jnp.concatenate([mean, jnp.zeros((120, 2 * chunk_rows), F32)], axis=0))
        row_mean = spread[:, 0:1]
        inv = lax.rsqrt(spread[:, 1:2] - row_mean * row_mean + EPS)
        for j, c in enumerate(pairs[n]):
            rows, cut = slice(c * chunk_rows, (c + 1) * chunk_rows), slice(j * chunk_rows, (j + 1) * chunk_rows)
            a = (conv[rows, :] - row_mean[cut]) * inv[cut] * channel_gain[...]
            act[rows, :] = (a / (1.0 + jnp.exp(-a))).astype(BF)

    conv_pair(0)
    weights_out(*range(BEFORE, n_piece))


    drain(ids_all, ids_recv)
    ids_in = pltpu.make_async_copy(ids_all, ids_s, ids_sem)
    ids_in.start()
    smalls[3].wait()
    for n in range(4, 7):
        loads[n].wait()
    n_rc = R // RC
    RP = RC // pass_rows
    pass_local = R // pass_rows

    def norm_rows(i, part, parts):
        rows = slice(i * RC + part * RC // parts, i * RC + (part + 1) * RC // parts)
        x = sto[rows, :].astype(F32)
        y = x * lax.rsqrt(jnp.mean(x * x, axis=-1, keepdims=True) + EPS) * passage_gain[...]
        sto[rows, :] = y.astype(BF)

    for i in range(n_rc):
        norm_rows(i, 0, 1)
        here, slots = pl.ds(i * RP, RP), pl.ds(core * pass_local + i * RP, RP)
        def project(dst, at, weight, cols):
            dst[at] = mm(sto[i * RC:(i + 1) * RC, :], weight[:, cols]).astype(BF).reshape(RP, pass_rows, HW)

        project(k_stage, here, kw, theirs)
        project(v_stage, here, vw, theirs)
        remote(k_stage.at[here], k_all.at[slots], kv_send, kv_recv.at[0], "st", partner).start()
        remote(v_stage.at[here], v_all.at[slots], kv_send, kv_recv.at[1], "st", partner).start()
        relay_near(i)
        project(k_all, slots, kw, mine)
        project(v_all, slots, vw, mine)

    ids_in.wait()
    drain(k_stage, kv_recv.at[0])
    drain(v_stage, kv_recv.at[1])

    heads = local_heads // 2
    HD_ = HW // heads
    per_chip = 2 * pass_local
    chunk_blocks = block_count // n_tp
    clane = lax.broadcasted_iota(jnp.int32, (chunk_rows, 128), 1)
    scale = HD_ ** (-0.5)

    def order(i):
        return lax.rem(chip + 1 + i // 2, n_chip) * 2 + lax.rem(core + 1 - i % 2, 2)

    pieces = [(0, u, u + 1) for u in range(chunk_blocks)] + [(k, 0, chunk_blocks) for k in range(1, n_tp)]

    def piece_rows(n):
        k, first, last = pieces[n]
        at = pl.multiple_of(chunks[k] * chunk_rows + first * block_len, block_len)
        return pl.ds(at, (last - first) * block_len)

    def answer_copies(n, r):
        rows = piece_rows(n)
        return (
            remote(out_o.at[r, rows], ret_o.at[st, rows], o_send, o_recv.at[n], "st", r),
            remote(out_s.at[r, n], ret_s.at[st, n], s_send, s_recv.at[n], "st", r),
        )

    def attend(m):
        k, first, last = pieces[m]
        d = chunks[k]
        rows = chunk_ds(d)
        spare = jnp.zeros((chunk_rows - (last - first) * block_len, 1), F32)

        rs = [order(i) for i in range(n_st)]
        if first == 0:
            drain(q_all.at[0:n_st - 1, rows], q_recv.at[k])
        units = [(e, h, u) for e in range(n_st) for h in range(heads) for u in range(first, last)]
        place, values, scores, tops, dens, weights = {}, {}, {}, {}, {}, {}
        for e, h, u in units:
            r = rs[e]
            cols = slice(h * HD_, (h + 1) * HD_)
            b = d * chunk_blocks + u
            brow = pl.ds(pl.multiple_of(b * block_len, block_len), block_len)
            ks, vs, bias = [], [], []
            for j in range(per_block):
                p = ids_s[r, j, b] - chip * per_chip
                spread_p = jnp.full((1, pass_rows), p, jnp.int32)
                valid = jnp.logical_and(spread_p >= 0, spread_p < per_chip)
                bias.append(jnp.where(valid, 0.0, NEG))
                slot = jnp.clip(p, 0, per_chip - 1)
                ks.append(k_all[slot][:, cols])
                vs.append(functools.partial(lambda slot, cols: v_all[slot][:, cols], slot, cols))
            s = lax.dot_general(q_all[r, brow, cols], jnp.concatenate(ks, axis=0), (((1,), (1,)), ((), ())),
                                preferred_element_type=F32)
            scores[e, h, u] = s * scale + jnp.concatenate(bias, axis=1)
            values[e, h, u] = vs
            place[e, h, u] = (r, brow, cols)
        for e0 in range(0, n_st, 2):
            batch = [n for n in units if n[0] in (e0, e0 + 1)]
            for n in batch:
                tops[n] = jnp.maximum(jnp.max(scores[n], axis=1, keepdims=True), NEG / 2)
            for n in batch:
                exponent = jnp.exp(scores[n] - tops[n])
                dens[n] = jnp.sum(exponent, axis=1, keepdims=True)
                weights[n] = exponent.astype(BF)
            for n in batch:
                r, brow, cols = place[n]
                out_o[r, brow, cols] = mm(weights[n], jnp.concatenate([v() for v in values[n]], axis=0)).astype(BF)
            stats = jnp.zeros((chunk_rows, 128), F32)
            for e in range(2):
                for h in range(heads):
                    for at, parts in ((2 * h, tops), (2 * h + 1, dens)):
                        column = [parts[e0 + e, h, u] for u in range(first, last)]
                        column = jnp.concatenate(column + [spare] * (spare.shape[0] > 0), axis=0)
                        stats = jnp.where(clane == 8 * e + at, column, stats)
            turned = jnp.transpose(stats)
            for e in range(2):
                r = rs[e0 + e]
                out_s[r, m] = turned[8 * e:8 * e + 8]
                if e0 + e < n_st - 1:
                    for c in answer_copies(m, r):
                        c.start()

    halves = chunk_blocks
    for m in range(halves):
        attend(m)
    for c in q_copies(n_tp - 1):
        c.start()
    relay_near(2)
    conv_pair(1)
    relay_near(3)
    relay_far(0)
    attend(halves)
    relay_far(1)
    smalls[5].wait()
    smalls[6].wait()
    act_pair(0)
    loads[7].wait()
    loads[8].wait()

    SR = chunk_rows // SUB
    cuts = {1: (0, 2 * SR, 4 * SR, chunk_rows), 2: (0, chunk_rows // 2, chunk_rows)}
    NC = 512

    def piece(lane, u):
        d = chunks[(0, 0, 1, 2)[lane]]
        rows = pl.ds(pl.multiple_of(d * chunk_rows + u * SR, SR), SR)
        slot = (0, 1, 2, 0)[lane]
        to = (mate, across, across, mate)[lane]
        box = inbox.at[slot, pl.ds(u * SR, SR)]
        return rows, slot, remote(part.at[rows], box, r_send, r_recv.at[slot, u], "tp", to)

    def rows_copies(k, n):
        at, size = cuts[k][n], cuts[k][n + 1] - cuts[k][n]
        rows = pl.ds(pl.multiple_of(chunks[k] * chunk_rows + at, 2 * SR), size)
        cut = pl.ds(at, size)
        return (
            remote(act.at[rows], mate_act.at[k - 1, cut], a_send.at[0], a_recv.at[0, k - 1, n], "tp", mate),
            remote(att.at[k, cut], mate_att.at[k - 1, cut], a_send.at[1], a_recv.at[1, k - 1, n], "tp", mate),
        )

    def rows_out(k):
        @pl.when(outer)
        def _():
            for n in range(len(cuts[k]) - 1):
                for c in rows_copies(k, n):
                    c.start()

    def combine(m):
        k, first, last = pieces[m]
        rows = piece_rows(m)
        cut = slice(first * block_len, last * block_len)
        drain(ret_o.at[0:n_st - 1, rows], o_recv.at[m])
        drain(ret_s.at[0:n_st - 1, m], s_recv.at[m])
        ret_s[st, m] = out_s[st, m]
        stats = jnp.transpose(jnp.concatenate(
            [ret_s[c, m] for c in range(n_st)] + [jnp.zeros((128 - 8 * n_st, chunk_rows), F32)], axis=0))
        stats = stats[:(last - first) * block_len]
        ret_o[st, rows, :] = out_o[st, rows, :]
        for g in range(2):
            for h in range(heads):
                cols = slice(h * HD_, (h + 1) * HD_)
                at = [8 * (c * 2 + g) + 2 * h for c in range(n_chip)]
                best = functools.reduce(jnp.maximum, [stats[:, x:x + 1] for x in at])
                num, den = 0.0, 0.0
                for c in range(n_chip):
                    w = jnp.exp(stats[:, at[c]:at[c] + 1] - best)
                    num = num + w * ret_o[c * 2 + g, rows, cols].astype(F32)
                    den = den + w * stats[:, at[c] + 1:at[c] + 2]
                att[k, cut, (g * heads + h) * HD_:(g * heads + h + 1) * HD_] = (num / den).astype(BF)

    def own_partial(m):
        k, first, last = pieces[m]
        rows = piece_rows(m)
        cut = slice(first * block_len, last * block_len)
        for i in range(part.shape[1] // NC):
            cols = slice(i * NC, (i + 1) * NC)
            part[rows, cols] = (mm(act[rows, :], mo[:, cols]) + blend_gain[:, cols] * mm(att[k, cut], ao[:, cols])).astype(BF)

    def mate_rows(k, n):
        for c in rows_copies(k, n):
            c.wait_recv()
        cut = slice(cuts[k][n], cuts[k][n + 1])
        rows = pl.ds(pl.multiple_of(chunks[k] * chunk_rows + cuts[k][n], 2 * SR), cuts[k][n + 1] - cuts[k][n])
        for i in range(part.shape[1] // NC):
            cols = slice(i * NC, (i + 1) * NC)
            value = (mm(mate_act[k - 1, cut], mo2[:, cols])
                     + blend_gain[:, cols] * mm(mate_att[k - 1, cut], ao2[:, cols])).astype(BF)
            if k == 1:
                part[rows, cols] = (part[rows, cols].astype(F32) + value.astype(F32)).astype(BF)
            else:
                mate_part[cut, cols] = value

    def send(lane, *steps):
        for u in steps:
            piece(lane, u)[2].start()

    def onward(lane_in, lane_out, *steps):
        for u in steps:
            slot = (0, 1, 2, 0)[lane_in]
            piece(lane_in, u)[2].wait_recv()
            rows, _, copy = piece(lane_out, u)
            part[rows, :] = (part[rows, :].astype(F32) + inbox[slot, pl.ds(u * SR, SR), :].astype(F32)).astype(BF)
            copy.start()

    for m in range(halves):
        combine(m)
        own_partial(m)

        @pl.when(outer)
        def _(m=m):
            for u in range(m * SUB // halves, min((m + 1) * SUB // halves, EARLY)):
                piece(0, u)[2].start()

    relay_near(4)
    relay_far(2)
    attend(halves + 1)
    relay_near(5)
    act_pair(1)
    relay_far(3)

    @pl.when(inner)
    def _():
        onward(0, 1, 0)

    combine(halves)
    rows_out(1)

    @pl.when(outer)
    def _():
        send(0, *range(EARLY, SUB))

    @pl.when(inner)
    def _():
        own_partial(halves)
        onward(0, 1, 1)

    attend(halves + 2)

    @pl.when(inner)
    def _():
        onward(0, 1, 2)

    combine(halves + 1)
    rows_out(2)
    relay_far(4)

    @pl.when(inner)
    def _():
        onward(0, 1, 3)
        own_partial(halves + 1)
        onward(0, 1, *range(4, EARLY))

    relay_far(5)

    @pl.when(inner)
    def _():
        for n in range(2):
            drain(quarter, pass_recv.at[n])
        mate_rows(1, 0)
        send(2, 0, 1)
        mate_rows(1, 1)
        send(2, 2, 3)
        onward(1, 3, 0, 1)
        mate_rows(1, 2)

    combine(halves + 2)
    own_partial(halves + 2)

    @pl.when(inner)
    def _():
        send(2, *range(4, LATE))
        onward(1, 3, 2, 3)
        onward(0, 1, 5, 6)
        onward(1, 3, 4)
        onward(0, 1, 7)
        send(2, *range(LATE, SUB))
        mate_rows(2, 0)
        onward(1, 3, 5)
        mate_rows(2, 1)
        onward(1, 3, 6, 7)
        for u in range(SUB):
            rows = pl.ds(pl.multiple_of(tp * chunk_rows + u * SR, SR), SR)
            cut = pl.ds(u * SR, SR)
            piece(2, u)[2].wait_recv()
            out_ref[cut, :] = (part[rows, :].astype(F32) + mate_part[cut, :].astype(F32)
                               + inbox[2, cut, :].astype(F32)).astype(BF)

    @pl.when(outer)
    def _():
        for u in range(SUB):
            rows = pl.ds(pl.multiple_of(tp * chunk_rows + u * SR, SR), SR)
            cut = pl.ds(u * SR, SR)
            piece(3, u)[2].wait_recv()
            out_ref[cut, :] = (part[rows, :].astype(F32) + inbox[0, cut, :].astype(F32)).astype(BF)

    @pl.when(outer)
    def _():
        drain(quarter, w_send.at[0])
        drain(part.at[0:chunk_rows], r_send)
        drain(act.at[0:2 * chunk_rows], a_send.at[0])
        drain(att.at[0:2], a_send.at[1])

    @pl.when(inner)
    def _():
        for route in (1, 2, 3):
            drain(quarter, w_send.at[route])
        drain(part.at[0:3 * chunk_rows], r_send)

    drain(ids_all.at[0:n_st - 1], ids_send)
    drain(q_all.at[0:n_st - 1], q_send)
    drain(k_all, kv_send)
    drain(stat_all.at[0:n_tp - 1], stat_send)
    drain(out_o.at[0:n_st - 1], o_send)
    drain(out_s.at[0:n_st - 1], s_send)


def fused_local(
    tokens, store, passage_ids, mix_gain, glu_value, glu_gate, conv_taps, channel_gain, mix_out,
    query_gain, passage_gain, query_proj, key_proj, value_proj, attn_out, blend_gain,
):
    n_st = lax.axis_size("st")
    n_tp = lax.axis_size("tp")
    T, D = tokens.shape
    P_, PR, _ = store.shape
    R = P_ * PR
    W = query_proj.shape[1]
    HW = W // 2
    CL = glu_value.shape[1]
    nb, per_block = passage_ids.shape
    pad = 8 * pl.cdiv((conv_taps.shape[0] - 1) // 2, 8)
    DMA = pltpu.SemaphoreType.DMA
    n_ans = n_tp - 1 + nb // n_tp
    V = pltpu.VMEM
    kern = functools.partial(layer_kernel, n_st, n_tp, nb, per_block, T // nb, W // HD, SEQ_LEN, PR)
    hbm = pl.BlockSpec(memory_space=pl.ANY)
    vm = pl.BlockSpec(memory_space=pltpu.VMEM)
    return pl.pallas_call(
        kern,
        out_shape=pltpu.VMEM((T // n_tp, D), BF),
        in_specs=[hbm] * 16,
        out_specs=vm,
        scratch_shapes=[
            V((T, D), BF), V((R, D), BF), V((D, CL), BF), V((D, CL), BF), V((CL, D), BF),
            V((D, W), BF), V((D, W), BF), V((D, W), BF), V((W, D), BF), DMA((9,)),
            V((per_block, nb), jnp.int32), V((1, D), F32), V(conv_taps.shape, BF), V((1, CL), F32), V((1, D), F32),
            V((1, D), F32), V((1, D), F32), DMA((7,)),
            V((n_st, per_block, nb), jnp.int32), pltpu.SMEM((n_st, per_block, nb), jnp.int32),
            DMA, DMA, DMA,
            V((n_st, T, HW), BF), V((T, HW), BF), DMA, DMA((n_tp,)),
            V((2 * P_, PR, HW), BF), V((2 * P_, PR, HW), BF), V((P_, PR, HW), BF), V((P_, PR, HW), BF),
            DMA, DMA((2,)),
            V((T // SEQ_LEN, SEQ_LEN + 2 * pad, CL), F32), V((T, CL), F32), V((T, 128), F32),
            V((n_tp, 2, 8, 2 * T // n_tp), F32), DMA, DMA((2,)), V((T, CL), BF),
            V((n_st, T, HW), BF), V((n_st, n_ans, 8, T // n_tp), F32), V((n_st, T, HW), BF),
            V((n_st, n_ans, 8, T // n_tp), F32),
            DMA, DMA((n_ans,)), DMA, DMA((n_ans,)),
            V((T, D), BF), V((3, T // n_tp, D), BF), DMA, DMA((3, SUB)),
            V((n_tp, T // n_tp, W), BF), V((2, T // n_tp, CL), BF), V((2, T // n_tp, W), BF),
            DMA((2,)), DMA((2, 2, 3)), V((T // n_tp, D), BF), V((CL, D), BF), V((W, D), BF),
            DMA((4,)), DMA(((W + CL) // 128,)), DMA(((W + CL) // 128,)), DMA((2,)),
        ],
        compiler_params=pltpu.CompilerParams(
            collective_id=0, has_side_effects=True, vmem_limit_bytes=VMEM_MIB * 1024 * 1024),
        name="layer",
    )(
        tokens, store.reshape(R, D), passage_ids.T, mix_gain.reshape(1, D), glu_value, glu_gate, conv_taps,
        channel_gain.reshape(1, CL), mix_out, query_gain.reshape(1, D), passage_gain.reshape(1, D),
        query_proj, key_proj, value_proj, attn_out, blend_gain.reshape(1, D),
    )


def solution(mesh):
    in_specs = (
        P(("grp", "st"), None),
        P(("grp", "st"), None, None),
        P(("grp", "st"), None),
        P(),
        P(None, "tp"),
        P(None, "tp"),
        P(None, "tp"),
        P("tp"),
        P("tp", None),
        P(),
        P(),
        P(None, "tp"),
        P(None, "tp"),
        P(None, "tp"),
        P("tp", None),
        P(),
    )
    out_specs = P(("grp", "st", "tp"), None)
    def body(*args):
        even = args[11].shape[1] // HD % 2 == 0 and mesh.shape["st"] % 2 == 0
        even = even and args[2].shape[0] % mesh.shape["tp"] == 0 and mesh.shape["st"] <= 16
        even = even and mesh.shape["tp"] == 4 and mesh.shape["grp"] == 2 and mesh.shape["st"] == 4 and args[2].shape[0] // mesh.shape["tp"] == 2
        even = even and args[0].shape[0] % (SEQ_LEN * mesh.shape["tp"]) == 0
        return (fused_local if even else local)(*args)

    return jax.shard_map(body, mesh=mesh, in_specs=in_specs, out_specs=out_specs, check_vma=False)
```
